256 devices in a mesh: grp: 2 (over y), fs: 32 (over z, core), tp: 4 (over x).
Axes of the slice: x: 4, y: 2, z: 16, core: 2. Of those that a mesh axis runs over, the one named last changes fastest.
The devices are a block of a 4x16x16 slice.
Arguments:
- tokens: bfloat16 [1536, 2048], P(('grp', 'tp')), parts along dimension 0, may hold values from -6 to 6
- norm_gain: float32 [2048], P('fs'), may hold values from 0.1 to 1.9
- up_trained: float32 [2048, 8192], P('fs', 'tp'), may hold values from -0.125 to 0.125
- down_trained: float32 [2048, 8192], P('fs', 'tp'), may hold values from -0.125 to 0.125
Outputs:
- up_serving: bfloat16 [4096, 8192], P('grp', 'fs'), parts along dimension 0
- down_serving: bfloat16 [4096, 8192], P('grp', 'fs'), parts along dimension 0
- prompt_output: bfloat16 [1536, 2048], P(('grp', 'tp'), 'fs'), parts along dimension 0
The draws below stay inside these ranges and needn't reach their ends.
There are 2 independent parts, one for each index of `grp`. The reference program is written for one: setup_inputs(seed, part) draws one part's arguments, and reference() takes and returns one part's arrays. A program takes and returns all parts, laid end to end along the dimension named above; an argument that names none is the same for every part. Nothing has to cross between parts.
All inputs are finite; a program needn't handle non-finite values.
Results may differ from the reference program's by a relative error of at most 0.0074.
Values may be sent and summed in bfloat16 or wider, within the bound.
A program may use at most 64 MiB of HBM per device.

```python
import jax
import jax.numpy as jnp
from jax import lax

D = 2048
FF = 8192
TOKENS = 768


def with_spikes(entries, stream_key, source, target, parts, factor):
    owner, partner = [(jnp.arange(entries.shape[axis_at]) // (entries.shape[axis_at] // parts)).reshape([-1 if axis == axis_at else 1 for axis in range(entries.ndim)]) for axis_at in (source, target)]
    chosen = jax.random.permutation(stream_key, parts)[partner]
    strong = (owner == chosen) | (owner == (partner + parts // 2) % parts)
    return jnp.where(strong, factor * entries, entries)


def levels(rng, extent, shards, least, top_value):
    def one(dim, blocks):
        heights = jax.random.uniform(jax.random.fold_in(jax.random.fold_in(rng, 6), dim), (blocks,), jnp.float32, least / len(shards), top_value / len(shards))
        return jnp.repeat(jnp.exp(heights), extent[dim] // blocks).reshape((-1,) + (1,) * (len(extent) - dim - 1))

    factor_of = one(*shards[0])
    for cut in shards[1:]:
        factor_of = factor_of * one(*cut)
    return factor_of


def normal_values(rng, shape, spread, most, shards=(), dtype=jnp.bfloat16):
    entries = jax.random.normal(rng, shape, jnp.float32) * spread
    if len(shards) > 0:
        entries = levels(rng, shape, shards, -0.22, 0.18) * entries
    return jnp.clip(entries, min=-most, max=most).astype(dtype)


def bell_draw_with(stream_key, extent, scale, reach, cuts, heavy, kind=jnp.bfloat16):
    entries = scale * jax.random.normal(stream_key, extent, jnp.float32)
    if cuts:
        entries = entries * levels(stream_key, extent, cuts, -0.22, 0.18)
    return jnp.clip(with_spikes(entries, jax.random.fold_in(stream_key, 3), *heavy), -reach, reach).astype(kind)


def setup_inputs(seed: int = 0, part: int = 0) -> dict:
    streams_of = jax.random.split(jax.random.key(seed), 5)
    own_keys = jax.random.split(jax.random.fold_in(streams_of[4], part), 5)
    return {
        "tokens": normal_values(own_keys[0], (TOKENS, D), 1.0, 6.0, ((0, 4),)),
        "norm_gain": jnp.clip(1.0 + 0.18 * jax.random.normal(streams_of[1], (D,), jnp.float32), 0.1, 1.9),
        "up_trained": normal_values(streams_of[2], (D, FF), D ** -0.5, 0.125, ((0, 32), (1, 4)), jnp.float32),
        "down_trained": bell_draw_with(streams_of[3], (D, FF), FF ** -0.5, 0.125, ((0, 32), (1, 4)), (1, 0, 32, 2.75), jnp.float32),
    }


epsilon = 1e-06

def reference(tokens, norm_gain, up_trained, down_trained):
    up_serving = (norm_gain[:, None] * up_trained).astype(jnp.bfloat16)
    down_serving = down_trained.astype(jnp.bfloat16)
    values = tokens.astype(jnp.float32)
    scale = lax.rsqrt(lax.optimization_barrier(jnp.mean(values * values, axis=1, keepdims=True)) + epsilon)
    normed = (values * scale).astype(jnp.bfloat16)
    hidden = jnp.dot(normed, up_serving, preferred_element_type=jnp.float32)
    active = jnp.square(jax.nn.relu(hidden)).astype(jnp.bfloat16)
    prompt_output = jnp.dot(active, down_serving.T, preferred_element_type=jnp.float32).astype(jnp.bfloat16)
    return (up_serving, down_serving, prompt_output)
```

```python
import functools

import jax
import jax.numpy as jnp
from jax import lax
from jax.experimental import pallas as pl
from jax.experimental.pallas import tpu as pltpu
from jax.sharding import PartitionSpec as P

MESH = pl.DeviceIdType.MESH
epsilon = 1e-06


def ring_order(n):
    half = n // 2
    pairs = [d for d in range(half - 1, 5, -1)] + [4, 3, 1, 5, 2]
    slots = [half]
    first = {}
    for d in pairs:
        first[d] = len(slots)
        slots += [d, n - d]
    slots.append(0)
    return slots, first


def kernel(
    shards,
    planes,
    tok_hbm,
    gain_hbm,
    up_hbm,
    down_hbm,
    up_out,
    down_out,
    y_ref,
    tok,
    gain,
    raw,
    normed,
    src,
    relay,
    full,
    mine,
    give,
    got,
    sums,
    stage,
    final,
    in_sem,
    out_sem,
    p1_send,
    p1_recv,
    p2_send,
    full_recv,
    p3_send,
    p4_send,
    pair_send,
    pair_recv,
    sum_send,
    stage_recv,
    final_recv,
):
    f = lax.axis_index("fs")
    x = lax.axis_index("tp")
    n_z = shards // 2
    z = f // 2
    c = f % 2
    rows, width = full.shape[2], full.shape[3]
    per_plane = src.shape[2]
    blocks_here = planes * per_plane
    sources = shards // planes

    barrier = pltpu.get_barrier_semaphore()
    for step in range(1, planes):
        pl.semaphore_signal(barrier, inc=1, device_id={"tp": (x + step) % planes}, device_id_type=MESH)

    def greet(step, carry):
        pl.semaphore_signal(barrier, inc=1, device_id={"fs": (f + step) % shards}, device_id_type=MESH)
        return carry

    lax.fori_loop(1, shards, greet, 0)

    loads = [
        pltpu.make_async_copy(gain_hbm, gain, in_sem.at[0]),
        pltpu.make_async_copy(up_hbm, raw.at[0], in_sem.at[1]),
        pltpu.make_async_copy(down_hbm, raw.at[1], in_sem.at[2]),
        pltpu.make_async_copy(tok_hbm, tok, in_sem.at[3]),
    ]
    for load in loads:
        load.start()

    def first_block(plane):
        return (plane + 4 * planes - z - 2 * c + shards * planes) % planes

    loads[0].wait()
    row_at = lax.broadcasted_iota(jnp.int32, (rows, rows), 0)
    col_at = lax.broadcasted_iota(jnp.int32, (rows, rows), 1)
    column = jnp.sum(
        jnp.where(row_at == col_at, jnp.broadcast_to(gain[...], (rows, rows)), 0.0), axis=1, keepdims=True
    )
    for kind in range(2):
        loads[1 + kind].wait()
        for plane in range(planes):
            for b in range(per_plane):
                at = pl.multiple_of((planes * b + first_block(plane)) * width, width)
                block = raw[kind, :, pl.ds(at, width)]
                if kind == 0:
                    block = block * column
                src[kind, plane, b] = block.astype(jnp.bfloat16)
    loads[3].wait()
    step_rows = 64
    for r in range(0, tok.shape[0], step_rows):
        values = tok[r : r + step_rows, :].astype(jnp.float32)
        scale = lax.rsqrt(jnp.mean(values * values, axis=1, keepdims=True) + epsilon)
        normed[r : r + step_rows, :] = (values * scale).astype(jnp.bfloat16)

    pl.semaphore_wait(barrier, planes - 1 + shards - 1)

    pending = []

    for kind in range(2):
        for step in (1, 3, 2):
            plane = (x + step) % planes
            copy = pltpu.make_async_remote_copy(
                src_ref=src.at[kind, plane],
                dst_ref=relay.at[kind, x],
                send_sem=p1_send.at[kind, step - 1],
                recv_sem=p1_recv.at[kind, x],
                device_id={"tp": plane},
                device_id_type=MESH,
            )
            copy.start()
            pending.append((None, copy))

    s = first_block(x)
    for kind in range(2):
        for step in (0, 3, 1, 2):
            a = (x + step) % planes
            if step == 0:
                held = src.at[kind, x]
            else:
                held = relay.at[kind, a]
                pltpu.make_async_copy(src.at[kind, 0], held, p1_recv.at[kind, a]).wait()
            for b in range(per_plane):
                to = blocks_here * a + planes * b + s
                away = to != f
                copy = pltpu.make_async_remote_copy(
                    src_ref=held.at[b],
                    dst_ref=full.at[kind, f],
                    send_sem=p2_send.at[kind, step * per_plane + b],
                    recv_sem=full_recv.at[kind, f],
                    device_id={"fs": to},
                    device_id_type=MESH,
                )
                pl.when(away)(copy.start)
                pending.append((away, copy))

                @pl.when(jnp.logical_not(away))
                def _():
                    full[kind, f] = held[b]

    def source(plane, i):
        r = (plane + 2 * shards - f) % planes
        odd = (z + r) % 2
        near = (i + 1) // 2
        even_at = jnp.int32(2 * near if i % 2 else n_z - 2 * near)
        odd_at = jnp.int32(1 + 2 * (i // 2) if i % 2 == 0 else n_z - 1 - 2 * (i // 2))
        zs = (z + jnp.where(odd == 1, odd_at, even_at)) % n_z
        return 2 * zs + ((zs + planes - r) // 2) % 2

    def arrived(kind, at):
        return pltpu.make_async_copy(full.at[kind, at], full.at[kind, at], full_recv.at[kind, at])

    def forward(kind, at, step, sem):
        copy = pltpu.make_async_remote_copy(
            src_ref=full.at[kind, at],
            dst_ref=full.at[kind, at],
            send_sem=sem,
            recv_sem=full_recv.at[kind, at],
            device_id={"tp": (x + step) % planes},
            device_id_type=MESH,
        )
        copy.start()
        pending.append((None, copy))

    def collect(kind):
        for i in range(sources):
            at = source(x, i)
            pl.when(at != f)(arrived(kind, at).wait)
            forward(kind, at, 1, p3_send.at[kind, i, 0])
            forward(kind, at, 3, p3_send.at[kind, i, 1])
        for i in range(sources):
            for step, parity in ((3, 0), (1, 1)):
                at = source((x + step) % planes, i)
                arrived(kind, at).wait()
                if i % 2 == parity:
                    forward(kind, at, 4 - step, p4_send.at[kind, i])
        for i in range(sources):
            arrived(kind, source((x + 2) % planes, i)).wait()

    collect(0)
    put_up = pltpu.make_async_copy(full.at[0], up_out, out_sem.at[0])
    put_up.start()
    up = full[0].reshape(shards * rows, width)
    hidden = jnp.dot(normed[...], up, preferred_element_type=jnp.float32)
    active = jnp.square(jnp.maximum(hidden, 0.0)).astype(jnp.bfloat16)

    collect(1)
    put_down = pltpu.make_async_copy(full.at[1], down_out, out_sem.at[1])
    put_down.start()

    half = tok.shape[0] // 2
    low = lax.broadcasted_iota(jnp.int32, (half, 2 * rows), 1) < rows
    slots, first = ring_order(n_z)
    for slot, ahead in enumerate(slots):
        owner = (z + ahead) % n_z
        block = full[1, pl.ds(2 * owner, 2)].reshape(2 * rows, width)
        part = lax.dot_general(active, block, (((1,), (1,)), ((), ())), preferred_element_type=jnp.float32)
        top, bottom = part[:half], part[half:]
        even = jnp.where(low, top, pltpu.roll(bottom, rows, 1))
        odd = jnp.where(low, pltpu.roll(top, rows, 1), bottom)
        mine[slot] = jnp.where(c == 0, even, odd)
        give[slot] = jnp.where(c == 0, odd, even).astype(jnp.bfloat16)

    cut = first[1]
    pair = []
    for j, (start, stop) in enumerate(((0, cut), (cut, n_z))):
        copy = pltpu.make_async_remote_copy(
            src_ref=give.at[pl.ds(start, stop - start)],
            dst_ref=got.at[pl.ds(start, stop - start)],
            send_sem=pair_send.at[j],
            recv_sem=pair_recv.at[j],
            device_id={"fs": f + 1 - 2 * c},
            device_id_type=MESH,
        )
        copy.start()
        pair.append(copy)

    top_d = n_z // 2
    groups = [(5, list(range(6, top_d + 1)), list(range(6, top_d))), (2, [3, 4], [3, 4])]
    sign = 1 - 2 * c

    def place(side, d):
        if d == top_d:
            return 0
        return first[d] + (c if side == 0 else 1 - c)

    def toward(side, d):
        return (z + n_z + (sign if side == 0 else -sign) * d) % n_z

    def pass_on(slot, dst, recv, to_z, j):
        copy = pltpu.make_async_remote_copy(
            src_ref=sums.at[slot],
            dst_ref=dst,
            send_sem=sum_send.at[j],
            recv_sem=recv,
            device_id={"fs": 2 * to_z + c},
            device_id_type=MESH,
        )
        copy.start()
        pending.append((None, copy))

    pair[0].wait_recv()
    for slot in range(cut):
        sums[slot] = (mine[slot] + got[slot].astype(jnp.float32)).astype(jnp.bfloat16)
    order = []
    for agent, big, small in groups:
        for side, members in ((0, big), (1, small)):
            for d in members:
                order.append((d - agent, d, side, agent))
    stage_at = {}
    count = 0
    for _, d, side, agent in sorted(order, reverse=True):
        stage_at[(side, d)] = count
        pass_on(place(side, d), stage.at[count], stage_recv.at[count], toward(side, d - agent), count)
        count += 1

    pair[1].wait_recv()
    for side in range(2):
        slot = place(side, 1)
        sums[slot] = (mine[slot] + got[slot].astype(jnp.float32)).astype(jnp.bfloat16)
    for side in range(2):
        pass_on(place(side, 1), final.at[4 + side], final_recv.at[4 + side], toward(side, 1), count + 4 + side)
    for g, (agent, big, small) in enumerate(groups):
        for side, members in ((0, big), (1, small)):
            slot = place(side, agent)
            total = mine[slot] + got[slot].astype(jnp.float32)
            for d in members:
                j = stage_at[(side, d)]
                pltpu.make_async_copy(stage.at[j], stage.at[j], stage_recv.at[j]).wait()
                total = total + stage[j].astype(jnp.float32)
            sums[slot] = total.astype(jnp.bfloat16)
            k = 2 * g + side
            pass_on(slot, final.at[k], final_recv.at[k], toward(side, agent), count + k)
    own = n_z - 1
    total = mine[own] + got[own].astype(jnp.float32)
    for k in (4, 5, 2, 3, 0, 1):
        pltpu.make_async_copy(final.at[k], final.at[k], final_recv.at[k]).wait()
        total = total + final[k].astype(jnp.float32)
    total = total.astype(jnp.bfloat16)
    y_ref[0:half, :] = total[:, 0:rows]
    y_ref[half : 2 * half, :] = total[:, rows : 2 * rows]

    put_up.wait()
    put_down.wait()
    for copy in pair:
        copy.wait_send()
    for when, copy in pending:
        if when is None:
            copy.wait_send()
        else:
            pl.when(when)(copy.wait_send)


def local(shards, planes, tokens, norm_gain, up_trained, down_trained):
    rows, cols = up_trained.shape
    count, depth = tokens.shape
    width = cols * planes // shards
    per_plane = cols // width // planes
    n_z = shards // 2
    half = count // 2
    bf16, f32 = jnp.bfloat16, jnp.float32
    served = jax.ShapeDtypeStruct((shards, rows, width), bf16)
    dma = pltpu.SemaphoreType.DMA
    any_space = pl.BlockSpec(memory_space=pl.ANY)
    up, down, y = pl.pallas_call(
        functools.partial(kernel, shards, planes),
        out_shape=(served, served, jax.ShapeDtypeStruct((count, rows), bf16)),
        in_specs=[any_space] * 4,
        out_specs=(any_space, any_space, pl.BlockSpec(memory_space=pltpu.VMEM)),
        scratch_shapes=[
            pltpu.VMEM((count, depth), bf16),
            pltpu.VMEM((1, rows), f32),
            pltpu.VMEM((2, rows, cols), f32),
            pltpu.VMEM((count, depth), bf16),
            pltpu.VMEM((2, planes, per_plane, rows, width), bf16),
            pltpu.VMEM((2, planes, per_plane, rows, width), bf16),
            pltpu.VMEM((2, shards, rows, width), bf16),
            pltpu.VMEM((n_z, half, 2 * rows), f32),
            pltpu.VMEM((n_z, half, 2 * rows), bf16),
            pltpu.VMEM((n_z, half, 2 * rows), bf16),
            pltpu.VMEM((n_z, half, 2 * rows), bf16),
            pltpu.VMEM((n_z, half, 2 * rows), bf16),
            pltpu.VMEM((6, half, 2 * rows), bf16),
            dma((4,)),
            dma((2,)),
            dma((2, planes - 1)),
            dma((2, planes)),
            dma((2, planes * per_plane)),
            dma((2, shards)),
            dma((2, shards // planes, 2)),
            dma((2, shards // planes)),
            dma((2,)),
            dma((2,)),
            dma((n_z,)),
            dma((n_z,)),
            dma((6,)),
        ],
        compiler_params=pltpu.CompilerParams(
            collective_id=0, has_side_effects=True, vmem_limit_bytes=48 * 1024 * 1024
        ),
        name="handoff",
    )(tokens, norm_gain.reshape(1, rows), up_trained, down_trained)
    return (up.reshape(shards * rows, width), down.reshape(shards * rows, width), y)


def solution(mesh):
    in_specs = (P(("grp", "tp"), None), P("fs"), P("fs", "tp"), P("fs", "tp"))
    out_specs = (P("grp", "fs"), P("grp", "fs"), P(("grp", "tp"), "fs"))
    body = functools.partial(local, mesh.shape["fs"], mesh.shape["tp"])
    return jax.shard_map(body, mesh=mesh, in_specs=in_specs, out_specs=out_specs, check_vma=False)
```

```python
import functools

import jax
import jax.numpy as jnp
from jax import lax
from jax.experimental import pallas as pl
from jax.experimental.pallas import tpu as pltpu
from jax.sharding import PartitionSpec as P

MESH = pl.DeviceIdType.MESH
epsilon = 1e-06
ahead_by = 5


def ring_order(n):
    half = n // 2
    pairs = [d for d in range(half - 1, 5, -1)] + [4, 3, 1, 5, 2]
    slots = [half]
    first = {}
    for d in pairs:
        first[d] = len(slots)
        slots += [d, n - d]
    slots.append(0)
    return slots, first


def kernel(
    shards,
    planes,
    tok_hbm,
    gain_hbm,
    up_hbm,
    down_hbm,
    up_out,
    down_out,
    y_ref,
    tok,
    gain,
    raw,
    normed,
    src,
    relay,
    full,
    mine,
    give,
    got,
    sums,
    stage,
    final,
    in_sem,
    out_sem,
    p1_send,
    p1_recv,
    p2_send,
    full_recv,
    p3_send,
    p4_send,
    pair_send,
    pair_recv,
    sum_send,
    stage_recv,
    final_recv,
    token,
    ready,
):
    f = lax.axis_index("fs")
    x = lax.axis_index("tp")
    n_z = shards // 2
    z = f // 2
    c = f % 2
    rows, width = full.shape[2], full.shape[3]
    per_plane = src.shape[2]
    blocks_here = planes * per_plane
    sources = shards // planes

    last = n_z - 1
    barrier = pltpu.get_barrier_semaphore()
    for step in range(1, planes):
        pl.semaphore_signal(barrier, inc=1, device_id={"tp": (x + step) % planes}, device_id_type=MESH)
    pl.semaphore_signal(barrier, inc=1, device_id={"fs": f + 1 - 2 * c}, device_id_type=MESH)

    @pl.when(z > 0)
    def _():
        pl.semaphore_signal(barrier, inc=1, device_id={"fs": f - 2}, device_id_type=MESH)

    @pl.when(z < last)
    def _():
        pl.semaphore_signal(barrier, inc=1, device_id={"fs": f + 2}, device_id_type=MESH)

    loads = [
        pltpu.make_async_copy(gain_hbm, gain, in_sem.at[0]),
        pltpu.make_async_copy(up_hbm, raw.at[0], in_sem.at[1]),
        pltpu.make_async_copy(down_hbm, raw.at[1], in_sem.at[2]),
        pltpu.make_async_copy(tok_hbm, tok, in_sem.at[3]),
    ]
    for load in loads:
        load.start()

    def first_block(plane):
        return (plane + 4 * planes - z - 2 * c + shards * planes) % planes

    loads[0].wait()
    row_at = lax.broadcasted_iota(jnp.int32, (rows, rows), 0)
    col_at = lax.broadcasted_iota(jnp.int32, (rows, rows), 1)
    column = jnp.sum(
        jnp.where(row_at == col_at, jnp.broadcast_to(gain[...], (rows, rows)), 0.0), axis=1, keepdims=True
    )
    for kind in range(2):
        loads[1 + kind].wait()
        for plane in range(planes):
            for b in range(per_plane):
                at = pl.multiple_of((planes * b + first_block(plane)) * width, width)
                block = raw[kind, :, pl.ds(at, width)]
                if kind == 0:
                    block = block * column
                src[kind, plane, b] = block.astype(jnp.bfloat16)
        relay[kind, x] = src[kind, x]
    loads[3].wait()
    step_rows = 64
    for r in range(0, tok.shape[0], step_rows):
        values = tok[r : r + step_rows, :].astype(jnp.float32)
        scale = lax.rsqrt(jnp.mean(values * values, axis=1, keepdims=True) + epsilon)
        normed[r : r + step_rows, :] = (values * scale).astype(jnp.bfloat16)

    pl.semaphore_wait(barrier, planes + jnp.where(z > 0, 1, 0) + jnp.where(z < last, 1, 0))

    def spread(kind, step):
        plane = (x + step) % planes
        return pltpu.make_async_remote_copy(
            src_ref=src.at[kind, plane],
            dst_ref=relay.at[kind, x],
            send_sem=p1_send.at[kind, step - 1],
            recv_sem=p1_recv.at[kind, x],
            device_id={"tp": plane},
            device_id_type=MESH,
        )

    for kind in range(2):
        for step in (1, 3, 2):
            spread(kind, step).start()

    @pl.when(z > 0)
    def _():
        pl.semaphore_wait(token, 1)

    @pl.when(z < last)
    def _():
        pl.semaphore_signal(token, inc=1, device_id={"fs": f + 2}, device_id_type=MESH)

    def source(plane, i):
        r = (plane + 2 * shards - f) % planes
        zs = r % 2 + 2 * i
        return 2 * zs + ((zs + planes - r) // 2) % 2

    def tell(i, carry):
        at = source(x, i)

        @pl.when(at // 2 < z)
        def _():
            pl.semaphore_signal(ready.at[f], inc=1, device_id={"fs": at}, device_id_type=MESH)

        return carry

    lax.fori_loop(0, sources, tell, 0)

    s = first_block(x)

    def along(kind, k):
        to = planes * k + s
        return to, pltpu.make_async_remote_copy(
            src_ref=relay.at[kind, k // per_plane, k % per_plane],
            dst_ref=full.at[kind, f],
            send_sem=p2_send.at[kind, k],
            recv_sem=full_recv.at[kind, f],
            device_id={"fs": to},
            device_id_type=MESH,
        )

    def send(kind, k):
        a = k // per_plane
        to, copy = along(kind, k)

        @pl.when(jnp.logical_and(k % per_plane == 0, a != x))
        def _():
            pltpu.make_async_copy(src.at[kind, 0], relay.at[kind, a], p1_recv.at[kind, a]).wait()

        if kind == 0:

            @pl.when(to // 2 > z)
            def _():
                pl.semaphore_wait(ready.at[to], 1)

        pl.when(to != f)(copy.start)

        @pl.when(to == f)
        def _():
            full[kind, f] = relay[kind, a, k % per_plane]

    def arrived(kind, at):
        return pltpu.make_async_copy(full.at[kind, at], full.at[kind, at], full_recv.at[kind, at])

    def hop(kind, at, step, sem):
        return pltpu.make_async_remote_copy(
            src_ref=full.at[kind, at],
            dst_ref=full.at[kind, at],
            send_sem=sem,
            recv_sem=full_recv.at[kind, at],
            device_id={"tp": (x + step) % planes},
            device_id_type=MESH,
        )

    def forward(kind, i):
        at = source(x, i)
        pl.when(at != f)(arrived(kind, at).wait)
        hop(kind, at, 1, p3_send.at[kind, i, 0]).start()
        hop(kind, at, 3, p3_send.at[kind, i, 1]).start()

    def pass_along(kind, i):
        left = source((x + 3) % planes, i)
        right = source((x + 1) % planes, i)
        arrived(kind, left).wait()
        pl.when(i % 2 == 0)(hop(kind, left, 1, p4_send.at[kind, i]).start)
        arrived(kind, right).wait()
        pl.when(i % 2 == 1)(hop(kind, right, 3, p4_send.at[kind, i]).start)

    def loop(count, body):
        def step(i, carry):
            body(i)
            return carry

        lax.fori_loop(0, count, step, 0)

    reach = z + ahead_by
    for kind in range(2):

        def near(j, kind=kind):
            t = j // per_plane
            a = (x + jnp.where(t == 1, 3, jnp.where(t == 0, 0, t - 1))) % planes
            k = a * per_plane + j % per_plane
            pl.when((planes * k + s) // 2 <= reach)(lambda: send(kind, k))

        loop(sources, near)
    for kind in range(2):

        def near_forward(i, kind=kind):
            pl.when(2 * i <= reach)(lambda: forward(kind, i))

        def near_pass(i, kind=kind):
            pl.when(2 * i <= reach)(lambda: pass_along(kind, i))

        loop(sources, near_forward)
        loop(sources, near_pass)

    def far(k):
        @pl.when(jnp.logical_and(k < sources, (planes * k + s) // 2 > reach))
        def _():
            send(0, k)
            send(1, k)

        @pl.when(jnp.logical_and(jnp.logical_and(k >= 1, k <= sources), 2 * (k - 1) > reach))
        def _():
            forward(0, k - 1)
            forward(1, k - 1)

        @pl.when(jnp.logical_and(k >= 2, 2 * (k - 2) > reach))
        def _():
            pass_along(0, k - 2)
            pass_along(1, k - 2)

    loop(sources + 2, far)

    def collect(kind):
        loop(sources, lambda i: arrived(kind, source((x + 2) % planes, i)).wait())

    pending = []
    collect(0)
    put_up = pltpu.make_async_copy(full.at[0], up_out, out_sem.at[0])
    put_up.start()
    up = full[0].reshape(shards * rows, width)
    hidden = jnp.dot(normed[...], up, preferred_element_type=jnp.float32)
    active = jnp.square(jnp.maximum(hidden, 0.0)).astype(jnp.bfloat16)

    collect(1)
    put_down = pltpu.make_async_copy(full.at[1], down_out, out_sem.at[1])
    put_down.start()

    half = tok.shape[0] // 2
    low = lax.broadcasted_iota(jnp.int32, (half, 2 * rows), 1) < rows
    slots, first = ring_order(n_z)
    for slot, ahead in enumerate(slots):
        owner = (z + ahead) % n_z
        block = full[1, pl.ds(2 * owner, 2)].reshape(2 * rows, width)
        part = lax.dot_general(active, block, (((1,), (1,)), ((), ())), preferred_element_type=jnp.float32)
        top, bottom = part[:half], part[half:]
        even = jnp.where(low, top, pltpu.roll(bottom, rows, 1))
        odd = jnp.where(low, pltpu.roll(top, rows, 1), bottom)
        mine[slot] = jnp.where(c == 0, even, odd)
        give[slot] = jnp.where(c == 0, odd, even).astype(jnp.bfloat16)

    cut = first[1]
    pair = []
    for j, (start, stop) in enumerate(((0, cut), (cut, n_z))):
        copy = pltpu.make_async_remote_copy(
            src_ref=give.at[pl.ds(start, stop - start)],
            dst_ref=got.at[pl.ds(start, stop - start)],
            send_sem=pair_send.at[j],
            recv_sem=pair_recv.at[j],
            device_id={"fs": f + 1 - 2 * c},
            device_id_type=MESH,
        )
        copy.start()
        pair.append(copy)

    top_d = n_z // 2
    groups = [(5, list(range(6, top_d + 1)), list(range(6, top_d))), (2, [3, 4], [3, 4])]
    sign = 1 - 2 * c

    def place(side, d):
        if d == top_d:
            return 0
        return first[d] + (c if side == 0 else 1 - c)

    def toward(side, d):
        return (z + n_z + (sign if side == 0 else -sign) * d) % n_z

    def pass_on(slot, dst, recv, to_z, j):
        copy = pltpu.make_async_remote_copy(
            src_ref=sums.at[slot],
            dst_ref=dst,
            send_sem=sum_send.at[j],
            recv_sem=recv,
            device_id={"fs": 2 * to_z + c},
            device_id_type=MESH,
        )
        copy.start()
        pending.append(copy)

    pair[0].wait_recv()
    for slot in range(cut):
        sums[slot] = (mine[slot] + got[slot].astype(jnp.float32)).astype(jnp.bfloat16)
    order = []
    for agent, big, small in groups:
        for side, members in ((0, big), (1, small)):
            for d in members:
                order.append((d - agent, d, side, agent))
    stage_at = {}
    count = 0
    for _, d, side, agent in sorted(order, reverse=True):
        stage_at[(side, d)] = count
        pass_on(place(side, d), stage.at[count], stage_recv.at[count], toward(side, d - agent), count)
        count += 1

    pair[1].wait_recv()
    for side in range(2):
        slot = place(side, 1)
        sums[slot] = (mine[slot] + got[slot].astype(jnp.float32)).astype(jnp.bfloat16)
    for side in range(2):
        pass_on(place(side, 1), final.at[4 + side], final_recv.at[4 + side], toward(side, 1), count + 4 + side)
    for g, (agent, big, small) in enumerate(groups):
        for side, members in ((0, big), (1, small)):
            slot = place(side, agent)
            total = mine[slot] + got[slot].astype(jnp.float32)
            for d in members:
                j = stage_at[(side, d)]
                pltpu.make_async_copy(stage.at[j], stage.at[j], stage_recv.at[j]).wait()
                total = total + stage[j].astype(jnp.float32)
            sums[slot] = total.astype(jnp.bfloat16)
            k = 2 * g + side
            pass_on(slot, final.at[k], final_recv.at[k], toward(side, agent), count + k)
    own = n_z - 1
    total = mine[own] + got[own].astype(jnp.float32)
    for k in (4, 5, 2, 3, 0, 1):
        pltpu.make_async_copy(final.at[k], final.at[k], final_recv.at[k]).wait()
        total = total + final[k].astype(jnp.float32)
    total = total.astype(jnp.bfloat16)
    y_ref[0:half, :] = total[:, 0:rows]
    y_ref[half : 2 * half, :] = total[:, rows : 2 * rows]

    put_up.wait()
    put_down.wait()
    for kind in range(2):
        for step in (1, 3, 2):
            spread(kind, step).wait_send()

        def drain(i, kind=kind):
            to, copy = along(kind, i)
            pl.when(to != f)(copy.wait_send)
            at = source(x, i)
            hop(kind, at, 1, p3_send.at[kind, i, 0]).wait_send()
            hop(kind, at, 3, p3_send.at[kind, i, 1]).wait_send()
            hop(kind, at, 1, p4_send.at[kind, i]).wait_send()

        loop(sources, drain)
    for copy in pair:
        copy.wait_send()
    for copy in pending:
        copy.wait_send()


def local(shards, planes, tokens, norm_gain, up_trained, down_trained):
    rows, cols = up_trained.shape
    count, depth = tokens.shape
    width = cols * planes // shards
    per_plane = cols // width // planes
    n_z = shards // 2
    half = count // 2
    bf16, f32 = jnp.bfloat16, jnp.float32
    served = jax.ShapeDtypeStruct((shards, rows, width), bf16)
    dma = pltpu.SemaphoreType.DMA
    any_space = pl.BlockSpec(memory_space=pl.ANY)
    up, down, y = pl.pallas_call(
        functools.partial(kernel, shards, planes),
        out_shape=(served, served, jax.ShapeDtypeStruct((count, rows), bf16)),
        in_specs=[any_space] * 4,
        out_specs=(any_space, any_space, pl.BlockSpec(memory_space=pltpu.VMEM)),
        scratch_shapes=[
            pltpu.VMEM((count, depth), bf16),
            pltpu.VMEM((1, rows), f32),
            pltpu.VMEM((2, rows, cols), f32),
            pltpu.VMEM((count, depth), bf16),
            pltpu.VMEM((2, planes, per_plane, rows, width), bf16),
            pltpu.VMEM((2, planes, per_plane, rows, width), bf16),
            pltpu.VMEM((2, shards, rows, width), bf16),
            pltpu.VMEM((n_z, half, 2 * rows), f32),
            pltpu.VMEM((n_z, half, 2 * rows), bf16),
            pltpu.VMEM((n_z, half, 2 * rows), bf16),
            pltpu.VMEM((n_z, half, 2 * rows), bf16),
            pltpu.VMEM((n_z, half, 2 * rows), bf16),
            pltpu.VMEM((6, half, 2 * rows), bf16),
            dma((4,)),
            dma((2,)),
            dma((2, planes - 1)),
            dma((2, planes)),
            dma((2, planes * per_plane)),
            dma((2, shards)),
            dma((2, shards // planes, 2)),
            dma((2, shards // planes)),
            dma((2,)),
            dma((2,)),
            dma((n_z,)),
            dma((n_z,)),
            dma((6,)),
            pltpu.SemaphoreType.REGULAR,
            pltpu.SemaphoreType.REGULAR((shards,)),
        ],
        compiler_params=pltpu.CompilerParams(
            collective_id=0, has_side_effects=True, vmem_limit_bytes=63 * 1024 * 1024
        ),
        name="handoff",
    )(tokens, norm_gain.reshape(1, rows), up_trained, down_trained)
    return (up.reshape(shards * rows, width), down.reshape(shards * rows, width), y)


def solution(mesh):
    in_specs = (P(("grp", "tp"), None), P("fs"), P("fs", "tp"), P("fs", "tp"))
    out_specs = (P("grp", "fs"), P("grp", "fs"), P(("grp", "tp"), "fs"))
    body = functools.partial(local, mesh.shape["fs"], mesh.shape["tp"])
    return jax.shard_map(body, mesh=mesh, in_specs=in_specs, out_specs=out_specs, check_vma=False)
```

```python
import functools

import jax
import jax.numpy as jnp
from jax import lax
from jax.experimental import pallas as pl
from jax.experimental.pallas import tpu as pltpu
from jax.sharding import PartitionSpec as P

MESH = pl.DeviceIdType.MESH
epsilon = 1e-06


def ring_order(n):
    half = n // 2
    far = [d for d in range(half - 1, 3, -1)]
    slots, first = [half], {half: 0}
    for d in far + [2, 1, 3]:
        first[d] = len(slots)
        slots += [d, n - d]
    slots.append(0)
    return slots, first, 1 + 2 * len(far)


def kernel(
    shards,
    planes,
    tok_hbm,
    gain_hbm,
    up_hbm,
    down_hbm,
    up_out,
    down_out,
    y_ref,
    tok,
    gain,
    raw,
    normed,
    src,
    relay,
    full,
    mine,
    give,
    got,
    sums,
    stage,
    in_sem,
    out_sem,
    p1_send,
    p1_recv,
    p2_send,
    full_recv,
    p3_send,
    p4_send,
    pair_send,
    pair_recv,
    sum_send,
    stage_recv,
):
    f = lax.axis_index("fs")
    x = lax.axis_index("tp")
    n_z = shards // 2
    z = f // 2
    c = f % 2
    rows, width = full.shape[2], full.shape[3]

    def around(v, n):
        v = jnp.where(v >= n, v - n, v)
        return jnp.where(v < 0, v + n, v)

    per_plane = src.shape[2]
    blocks_here = planes * per_plane
    sources = shards // planes

    barrier = pltpu.get_barrier_semaphore()
    for step in range(1, planes):
        pl.semaphore_signal(barrier, inc=1, device_id={"tp": around(x + step, planes)}, device_id_type=MESH)

    def greet(step, carry):
        pl.semaphore_signal(barrier, inc=1, device_id={"fs": around(f + step, shards)}, device_id_type=MESH)
        return carry

    lax.fori_loop(1, shards, greet, 0)

    loads = [
        pltpu.make_async_copy(gain_hbm, gain, in_sem.at[0]),
        pltpu.make_async_copy(up_hbm, raw.at[0], in_sem.at[1]),
        pltpu.make_async_copy(down_hbm, raw.at[1], in_sem.at[2]),
        pltpu.make_async_copy(tok_hbm, tok, in_sem.at[3]),
    ]
    for load in loads:
        load.start()

    turn = (shards * planes - z - 2 * c) % planes

    def first_block(plane):
        return around(plane + turn, planes)

    loads[0].wait()
    row_at = lax.broadcasted_iota(jnp.int32, (rows, rows), 0)
    col_at = lax.broadcasted_iota(jnp.int32, (rows, rows), 1)
    column = jnp.sum(
        jnp.where(row_at == col_at, jnp.broadcast_to(gain[...], (rows, rows)), 0.0), axis=1, keepdims=True
    )

    def fold(kind):
        loads[1 + kind].wait()
        for step in (1, 3, 2, 0):
            plane = around(x + step, planes)
            for b in range(per_plane):
                at = pl.multiple_of((planes * b + first_block(plane)) * width, width)
                block = raw[kind, :, pl.ds(at, width)]
                if kind == 0:
                    block = block * column
                src[kind, plane, b] = block.astype(jnp.bfloat16)

    def norm():
        loads[3].wait()
        step_rows = 64
        for r in range(0, tok.shape[0], step_rows):
            values = tok[r : r + step_rows, :].astype(jnp.float32)
            scale = lax.rsqrt(jnp.mean(values * values, axis=1, keepdims=True) + epsilon)
            normed[r : r + step_rows, :] = (values * scale).astype(jnp.bfloat16)

    fold(0)
    fold(1)
    pl.semaphore_wait(barrier, planes - 1 + shards - 1)

    pending = []

    for kind in range(2):
        for step in (1, 3, 2):
            plane = around(x + step, planes)
            copy = pltpu.make_async_remote_copy(
                src_ref=src.at[kind, plane],
                dst_ref=relay.at[kind, x],
                send_sem=p1_send.at[kind, step - 1],
                recv_sem=p1_recv.at[kind, x],
                device_id={"tp": plane},
                device_id_type=MESH,
            )
            copy.start()
            pending.append((None, copy))

    s = first_block(x)
    lift = s // 2

    def taken(kind, a):
        pltpu.make_async_copy(src.at[kind, 0], relay.at[kind, a], p1_recv.at[kind, a]).wait()

    def along(kind, k, held, n):
        to = planes * k + s
        away = to != f
        copy = pltpu.make_async_remote_copy(
            src_ref=held,
            dst_ref=full.at[kind, f],
            send_sem=p2_send.at[kind, n],
            recv_sem=full_recv.at[kind, f],
            device_id={"fs": to},
            device_id_type=MESH,
        )
        pl.when(away)(copy.start)
        pending.append((away, copy))

        @pl.when(jnp.logical_not(away))
        def _():
            full[kind, f] = held[...]

    for step in (0, 3, 1, 2):
        a = around(x + step, planes)
        if step > 0:
            taken(0, a)
        for b in range(per_plane):
            held = src.at[0, x, b] if step == 0 else relay.at[0, a, b]
            along(0, per_plane * a + b, held, step * per_plane + b)

    relay[1, x] = src[1, x]
    norm()

    hops = [2 * ((i + 1) // 2) if i % 2 == 0 else -2 * ((i + 1) // 2) for i in range(sources)]

    def sources_of(plane):
        r = (plane + 2 * shards - f) % planes
        odd = (z + r) % 2
        base = ((z + odd + planes - r) // 2) % 2
        found = []
        for ahead in hops:
            core = base if (ahead // 2) % 2 == 0 else 1 - base
            found.append(2 * around(z + odd + ahead, n_z) + core)
        return found

    own, right, across, left = [sources_of(around(x + step, planes)) for step in range(planes)]
    beyond = list(range(sources - 1, -1, -1))

    def arrived(kind, at):
        return pltpu.make_async_copy(full.at[kind, at], full.at[kind, at], full_recv.at[kind, at])

    def forward(kind, at, step, sem):
        copy = pltpu.make_async_remote_copy(
            src_ref=full.at[kind, at],
            dst_ref=full.at[kind, at],
            send_sem=sem,
            recv_sem=full_recv.at[kind, at],
            device_id={"tp": around(x + step, planes)},
            device_id_type=MESH,
        )
        copy.start()
        pending.append((None, copy))

    def to_sides(kind, some):
        for i in some:
            at = own[i]
            pl.when(at != f)(arrived(kind, at).wait)
            forward(kind, at, 1, p3_send.at[kind, i, 0])
            forward(kind, at, 3, p3_send.at[kind, i, 1])

    def from_sides(kind, some):
        for i in some:
            for found, step, parity in ((left, 1, 0), (right, 3, 1)):
                at = found[i]
                arrived(kind, at).wait()
                if i % 2 == parity:
                    forward(kind, at, step, p4_send.at[kind, i])

    def from_across(kind, some):
        for i in some:
            arrived(kind, across[i]).wait()

    near_at = jnp.where(z < lift, lift - z, z - lift) % 2
    near = z + near_at
    for a in range(planes):
        pl.when(a != x)(functools.partial(taken, 1, a))
    for n, i in enumerate(beyond):
        k = (around(near + hops[i], n_z) - lift) // 2
        along(1, k, relay.at[1, k // per_plane, k % per_plane], n)

    everything = list(range(sources))
    to_sides(0, everything)
    from_sides(0, everything)
    from_across(0, everything)
    put_up = pltpu.make_async_copy(full.at[0], up_out, out_sem.at[0])
    put_up.start()
    up = full[0].reshape(shards * rows, width)
    hidden = jnp.dot(normed[...], up, preferred_element_type=jnp.float32)
    active = jnp.square(jnp.maximum(hidden, 0.0)).astype(jnp.bfloat16)

    half = tok.shape[0] // 2
    low = lax.broadcasted_iota(jnp.int32, (half, 2 * rows), 1) < rows
    slots, first, cut = ring_order(n_z)

    def part_of(slot):
        owner = around(z + slots[slot], n_z)
        block = full[1, pl.ds(2 * owner, 2)].reshape(2 * rows, width)
        part = lax.dot_general(active, block, (((1,), (1,)), ((), ())), preferred_element_type=jnp.float32)
        top, bottom = part[:half], part[half:]
        even = jnp.where(low, top, pltpu.roll(bottom, rows, 1))
        odd = jnp.where(low, pltpu.roll(top, rows, 1), bottom)
        mine[slot] = jnp.where(c == 0, even, odd)
        give[slot] = jnp.where(c == 0, odd, even).astype(jnp.bfloat16)

    def exchange(j, start, stop):
        copy = pltpu.make_async_remote_copy(
            src_ref=give.at[pl.ds(start, stop - start)],
            dst_ref=got.at[pl.ds(start, stop - start)],
            send_sem=pair_send.at[j],
            recv_sem=pair_recv.at[j],
            device_id={"fs": f + 1 - 2 * c},
            device_id_type=MESH,
        )
        copy.start()
        pending.append((None, copy))
        return copy

    top_d = n_z // 2
    sign = 1 - 2 * c

    def place(side, d):
        if d == top_d:
            return 0
        return first[d] + (c if side == 0 else 1 - c)

    count = [0]
    stage_at = {}

    def pass_on(side, d, target):
        j = count[0]
        count[0] += 1
        stage_at[(side, d)] = j
        to = around(z + (sign if side == 0 else -sign) * (d - target), n_z)
        copy = pltpu.make_async_remote_copy(
            src_ref=sums.at[place(side, d)],
            dst_ref=stage.at[j],
            send_sem=sum_send.at[j],
            recv_sem=stage_recv.at[j],
            device_id={"fs": 2 * to + c},
            device_id_type=MESH,
        )
        copy.start()
        pending.append((None, copy))

    def add_up(side, d, below):
        slot = place(side, d)
        total = mine[slot] + got[slot].astype(jnp.float32)
        for e in below:
            j = stage_at[(side, e)]
            pltpu.make_async_copy(stage.at[j], stage.at[j], stage_recv.at[j]).wait()
            total = total + stage[j].astype(jnp.float32)
        return total

    def settle(side, d, below=()):
        sums[place(side, d)] = add_up(side, d, below).astype(jnp.bfloat16)

    far = beyond[:5]
    close = beyond[5:]
    to_sides(1, far)
    from_sides(1, far)
    from_across(1, far)
    for slot in range(cut):
        part_of(slot)
    pair_far = exchange(0, 0, cut)
    to_sides(1, close)
    pair_far.wait_recv()
    leaves = [(0, top_d, 6), (0, 7, 6), (1, 7, 6), (0, 5, 4), (1, 5, 4)]
    for side, d, target in leaves:
        settle(side, d)
    for side, d, target in leaves:
        pass_on(side, d, target)
    from_sides(1, close)
    from_across(1, close)
    put_down = pltpu.make_async_copy(full.at[1], down_out, out_sem.at[1])
    put_down.start()
    settle(0, 6, (top_d, 7))
    settle(1, 6, (7,))
    pass_on(0, 6, 3)
    pass_on(1, 6, 3)
    settle(0, 4, (5,))
    settle(1, 4, (5,))
    pass_on(0, 4, 3)
    pass_on(1, 4, 3)
    for slot in range(cut, n_z):
        part_of(slot)
    pair_near = exchange(1, cut, n_z)
    pair_near.wait_recv()
    for d in (2, 1):
        for side in range(2):
            settle(side, d)
    for d in (2, 1):
        for side in range(2):
            pass_on(side, d, 0)
    for side in range(2):
        settle(side, 3, (6, 4))
        pass_on(side, 3, 0)
    home = n_z - 1
    total = mine[home] + got[home].astype(jnp.float32)
    for d in (1, 2, 3):
        for side in range(2):
            j = stage_at[(side, d)]
            pltpu.make_async_copy(stage.at[j], stage.at[j], stage_recv.at[j]).wait()
            total = total + stage[j].astype(jnp.float32)
    total = total.T
    y_ref[:, 0:half] = total[0:rows].astype(jnp.bfloat16)
    y_ref[:, half : 2 * half] = total[rows : 2 * rows].astype(jnp.bfloat16)

    put_up.wait()
    put_down.wait()
    for when, copy in pending:
        if when is None:
            copy.wait_send()
        else:
            pl.when(when)(copy.wait_send)


def local(shards, planes, tokens, norm_gain, up_trained, down_trained):
    rows, cols = up_trained.shape
    count, depth = tokens.shape
    width = cols * planes // shards
    per_plane = cols // width // planes
    n_z = shards // 2
    half = count // 2
    bf16, f32 = jnp.bfloat16, jnp.float32
    served = jax.ShapeDtypeStruct((shards, rows, width), bf16)
    dma = pltpu.SemaphoreType.DMA
    any_space = pl.BlockSpec(memory_space=pl.ANY)
    up, down, y = pl.pallas_call(
        functools.partial(kernel, shards, planes),
        out_shape=(served, served, jax.ShapeDtypeStruct((rows, count), bf16)),
        in_specs=[any_space] * 4,
        out_specs=(any_space, any_space, pl.BlockSpec(memory_space=pltpu.VMEM)),
        scratch_shapes=[
            pltpu.VMEM((count, depth), bf16),
            pltpu.VMEM((1, rows), f32),
            pltpu.VMEM((2, rows, cols), f32),
            pltpu.VMEM((count, depth), bf16),
            pltpu.VMEM((2, planes, per_plane, rows, width), bf16),
            pltpu.VMEM((2, planes, per_plane, rows, width), bf16),
            pltpu.VMEM((2, shards, rows, width), bf16),
            pltpu.VMEM((n_z, half, 2 * rows), f32),
            pltpu.VMEM((n_z, half, 2 * rows), bf16),
            pltpu.VMEM((n_z, half, 2 * rows), bf16),
            pltpu.VMEM((n_z, half, 2 * rows), bf16),
            pltpu.VMEM((n_z, half, 2 * rows), bf16),
            dma((4,)),
            dma((2,)),
            dma((2, planes - 1)),
            dma((2, planes)),
            dma((2, planes * per_plane)),
            dma((2, shards)),
            dma((2, shards // planes, 2)),
            dma((2, shards // planes)),
            dma((2,)),
            dma((2,)),
            dma((n_z,)),
            dma((n_z,)),
        ],
        compiler_params=pltpu.CompilerParams(
            collective_id=0, has_side_effects=True, vmem_limit_bytes=63 * 1024 * 1024
        ),
        name="handoff",
    )(tokens, norm_gain.reshape(1, rows), up_trained, down_trained)
    return (up.reshape(shards * rows, width), down.reshape(shards * rows, width), y.T)


def solution(mesh):
    in_specs = (P(("grp", "tp"), None), P("fs"), P("fs", "tp"), P("fs", "tp"))
    out_specs = (P("grp", "fs"), P("grp", "fs"), P(("grp", "tp"), "fs"))
    body = functools.partial(local, mesh.shape["fs"], mesh.shape["tp"])
    return jax.shard_map(body, mesh=mesh, in_specs=in_specs, out_specs=out_specs, check_vma=False)
```

```python
import functools

import jax
import jax.numpy as jnp
from jax import lax
from jax.experimental import pallas as pl
from jax.experimental.pallas import tpu as pltpu
from jax.sharding import PartitionSpec as P

MESH = pl.DeviceIdType.MESH
epsilon = 1e-06
behind = 5.0


def ring_order(n):
    half = n // 2
    far = [d for d in range(half - 1, 3, -1)]
    slots, first = [half], {half: 0}
    for d in far + [2, 1, 3]:
        first[d] = len(slots)
        slots += [d, n - d]
    slots.append(0)
    return slots, first, 1 + 2 * len(far)


def kernel(
    shards,
    planes,
    tok_hbm,
    gain_hbm,
    up_hbm,
    down_hbm,
    up_out,
    down_out,
    y_ref,
    tok,
    gain,
    raw,
    normed,
    src,
    relay,
    mine,
    give,
    got,
    sums,
    stage,
    in_sem,
    p1_send,
    p1_recv,
    p2_send,
    full_recv,
    p3_send,
    p4_send,
    pair_send,
    pair_recv,
    sum_send,
    stage_recv,
    token,
    ready,
    active,
):
    f = lax.axis_index("fs")
    x = lax.axis_index("tp")
    n_z = shards // 2
    z = f // 2
    c = f % 2
    rows, width = up_out.shape[1], up_out.shape[2]

    full = (up_out, down_out)

    def when(flag):
        return (lambda body: body()) if flag is True else pl.when(flag)

    def both(a, b):
        return b if a is True else jnp.logical_and(a, b)

    def around(v, n):
        v = jnp.where(v >= n, v - n, v)
        return jnp.where(v < 0, v + n, v)

    per_plane = src.shape[2]
    blocks_here = planes * per_plane
    sources = shards // planes

    last = n_z - 1
    barrier = pltpu.get_barrier_semaphore()
    for step in range(1, planes):
        pl.semaphore_signal(barrier, inc=1, device_id={"tp": around(x + step, planes)}, device_id_type=MESH)
    pl.semaphore_signal(barrier, inc=1, device_id={"fs": f + 1 - 2 * c}, device_id_type=MESH)

    @pl.when(z == 0)
    def _():
        pl.semaphore_signal(barrier, inc=1, device_id={"fs": f + 2 * last}, device_id_type=MESH)

    loads = [
        pltpu.make_async_copy(gain_hbm, gain, in_sem.at[0]),
        pltpu.make_async_copy(up_hbm, raw.at[0], in_sem.at[1]),
        pltpu.make_async_copy(down_hbm, raw.at[1], in_sem.at[2]),
        pltpu.make_async_copy(tok_hbm, tok, in_sem.at[3]),
    ]
    for load in loads:
        load.start()

    turn = (shards * planes - z - 2 * c) % planes

    def first_block(plane):
        return around(plane + turn, planes)

    loads[0].wait()
    row_at = lax.broadcasted_iota(jnp.int32, (rows, rows), 0)
    col_at = lax.broadcasted_iota(jnp.int32, (rows, rows), 1)
    column = jnp.sum(
        jnp.where(row_at == col_at, jnp.broadcast_to(gain[...], (rows, rows)), 0.0), axis=1, keepdims=True
    )

    def fold(kind):
        loads[1 + kind].wait()
        for step in (1, 3, 2, 0):
            plane = around(x + step, planes)
            for b in range(per_plane):
                at = pl.multiple_of((planes * b + first_block(plane)) * width, width)
                block = raw[kind, :, pl.ds(at, width)]
                if kind == 0:
                    block = block * column
                src[kind, plane, b] = block.astype(jnp.bfloat16)

    def norm():
        loads[3].wait()
        step_rows = 64
        for r in range(0, tok.shape[0], step_rows):
            values = tok[r : r + step_rows, :].astype(jnp.float32)
            scale = lax.rsqrt(jnp.mean(values * values, axis=1, keepdims=True) + epsilon)
            normed[r : r + step_rows, :] = (values * scale).astype(jnp.bfloat16)

    pl.semaphore_wait(barrier, planes + jnp.where(z > 1, 1, 0) + jnp.where(z == last, 1, 0))

    @pl.when(jnp.logical_and(z > 0, z < last))
    def _():
        pl.semaphore_signal(barrier, inc=1, device_id={"fs": f + 2}, device_id_type=MESH)

    @pl.when(z == last)
    def _():
        pl.semaphore_signal(token, inc=1, device_id={"fs": f - 2 * last}, device_id_type=MESH)


    pending = []

    def spread(kind):
        fold(kind)
        for b in range(per_plane):
            for step in (1, 3, 2):
                plane = around(x + step, planes)
                copy = pltpu.make_async_remote_copy(
                    src_ref=src.at[kind, plane, b],
                    dst_ref=relay.at[kind, x, b],
                    send_sem=p1_send.at[kind, step - 1, b],
                    recv_sem=p1_recv.at[kind, x, b],
                    device_id={"tp": plane},
                    device_id_type=MESH,
                )
                copy.start()
                pending.append((None, copy))
        relay[kind, x] = src[kind, x]

    hops = [2 * ((i + 1) // 2) if i % 2 == 0 else -2 * ((i + 1) // 2) for i in range(sources)]

    def turn_of(plane):
        return (plane + 2 * shards - f) % planes

    def sources_of(plane):
        r = turn_of(plane)
        odd = (z + r) % 2
        base = ((z + odd + planes - r) // 2) % 2
        found = []
        for ahead in hops:
            core = base if (ahead // 2) % 2 == 0 else 1 - base
            found.append(2 * around(z + odd + ahead, n_z) + core)
        return found

    own, right, across, left = [sources_of(around(x + step, planes)) for step in range(planes)]
    beyond = list(range(sources - 1, -1, -1))
    def tell():
        for at in own:

            @pl.when(jnp.logical_and(at >= 2, jnp.logical_or(at < 2 * z, z == 0)))
            def _():
                pl.semaphore_signal(ready.at[f], inc=1, device_id={"fs": at}, device_id_type=MESH)

    pl.when(z > 0)(tell)
    spread(0)
    spread(1)

    @pl.when(z == 0)
    def _():
        pl.semaphore_wait(token, 1)
        tell()

    s = first_block(x)
    lift = s // 2

    def taken(kind, a, b):
        here = relay.at[kind, a, b]
        pltpu.make_async_copy(here, here, p1_recv.at[kind, a, b]).wait()

    def along(kind, a, b, n, wanted=True):
        to = blocks_here * a + planes * b + s
        away = both(wanted, to != f)
        held = relay.at[kind, a, b]
        copy = pltpu.make_async_remote_copy(
            src_ref=held,
            dst_ref=full[kind].at[f],
            send_sem=p2_send.at[kind, n],
            recv_sem=full_recv.at[kind, f],
            device_id={"fs": to},
            device_id_type=MESH,
        )
        pl.when(both(wanted, a != x))(lambda: taken(kind, a, b))
        if kind == 0:

            @pl.when(both(wanted, jnp.logical_and(z > 0, jnp.logical_or(to > 2 * z + 1, to < 2))))
            def _():
                pl.semaphore_wait(ready.at[to], 1)

        pl.when(away)(copy.start)
        pending.append((away, copy))

        @pl.when(both(wanted, to == f))
        def _():
            full[kind][f] = held[...]

    norm()

    def arrived(kind, at):
        return pltpu.make_async_copy(full[kind].at[at], full[kind].at[at], full_recv.at[kind, at])

    def forward(kind, at, step, sem):
        copy = pltpu.make_async_remote_copy(
            src_ref=full[kind].at[at],
            dst_ref=full[kind].at[at],
            send_sem=sem,
            recv_sem=full_recv.at[kind, at],
            device_id={"tp": around(x + step, planes)},
            device_id_type=MESH,
        )
        return copy

    early = n_z - n_z // 4
    late = list(range(sources, sources + sources // 4))

    def of_slot(step, i):
        if i < sources:
            at = (own, right, across, left)[step][i]
            return at, jnp.logical_and(at >= 2, at < 2 * early + 2)
        r = turn_of(around(x + step, planes))
        zs = around(early + 1 + 2 * (i - sources) + (r + early + 1) % 2, n_z)
        return 2 * zs + ((zs + planes - r) // 2) % 2, True

    def to_sides(kind, i):
        at, stands = of_slot(0, i)

        @when(stands)
        def _():
            pl.when(at != f)(lambda: arrived(kind, at).wait())
            forward(kind, at, 1, p3_send.at[kind, i, 0]).start()
            forward(kind, at, 3, p3_send.at[kind, i, 1]).start()

        pending.append((stands, forward(kind, at, 1, p3_send.at[kind, i, 0])))
        pending.append((stands, forward(kind, at, 3, p3_send.at[kind, i, 1])))

    def from_sides(kind, i):
        for from_step, to_step, parity in ((3, 1, 0), (1, 3, 1)):
            at, stands = of_slot(from_step, i)
            turned = (at // 4) % 2 == parity
            sem = p4_send.at[kind, i, parity]

            @when(stands)
            def _():
                arrived(kind, at).wait()
                pl.when(turned)(lambda: forward(kind, at, to_step, sem).start())

            pending.append((both(stands, turned), forward(kind, at, to_step, sem)))

    def from_across(kind, some):
        for i in some:
            at, stands = of_slot(2, i)
            when(stands)(lambda: arrived(kind, at).wait())

    near = z + jnp.where(z < lift, lift - z, z - lift) % 2
    everything = list(range(sources))
    for b in range(per_plane):
        along(0, x, b, sources + b)
    for kind, some in ((0, everything), (1, beyond)):
        for i in some:
            k = (around(near + hops[i], n_z) - lift) // 2
            a = k // per_plane
            along(kind, a, k % per_plane, i, a != x if kind == 0 else True)

    half = tok.shape[0] // 2
    low = lax.broadcasted_iota(jnp.int32, (half, 2 * rows), 1) < rows
    slots, first, cut = ring_order(n_z)

    def part_of(slot):
        owner = around(z + slots[slot], n_z)
        block = down_out[pl.ds(2 * owner, 2)].reshape(2 * rows, width)
        part = lax.dot_general(active[...], block, (((1,), (1,)), ((), ())), preferred_element_type=jnp.float32)
        top, bottom = part[:half], part[half:]
        even = jnp.where(low, top, pltpu.roll(bottom, rows, 1))
        odd = jnp.where(low, pltpu.roll(top, rows, 1), bottom)
        mine[slot] = jnp.where(c == 0, even, odd)
        give[slot] = jnp.where(c == 0, odd, even).astype(jnp.bfloat16)

    def exchange(j, start, stop):
        copy = pltpu.make_async_remote_copy(
            src_ref=give.at[pl.ds(start, stop - start)],
            dst_ref=got.at[pl.ds(start, stop - start)],
            send_sem=pair_send.at[j],
            recv_sem=pair_recv.at[j],
            device_id={"fs": f + 1 - 2 * c},
            device_id_type=MESH,
        )
        copy.start()
        pending.append((None, copy))
        return copy

    top_d = n_z // 2
    sign = 1 - 2 * c

    def place(side, d):
        if d == top_d:
            return 0
        return first[d] + (c if side == 0 else 1 - c)

    count = [0]
    stage_at = {}

    def pass_on(side, d, target):
        j = count[0]
        count[0] += 1
        stage_at[(side, d)] = j
        to = around(z + (sign if side == 0 else -sign) * (d - target), n_z)
        copy = pltpu.make_async_remote_copy(
            src_ref=sums.at[place(side, d)],
            dst_ref=stage.at[j],
            send_sem=sum_send.at[j],
            recv_sem=stage_recv.at[j],
            device_id={"fs": 2 * to + c},
            device_id_type=MESH,
        )
        copy.start()
        pending.append((None, copy))

    def add_up(side, d, below):
        slot = place(side, d)
        total = mine[slot] + got[slot].astype(jnp.float32)
        for e in below:
            j = stage_at[(side, e)]
            pltpu.make_async_copy(stage.at[j], stage.at[j], stage_recv.at[j]).wait()
            total = total + stage[j].astype(jnp.float32)
        return total

    def settle(side, d, below=()):
        sums[place(side, d)] = add_up(side, d, below).astype(jnp.bfloat16)

    far = beyond[:5] + late
    close = beyond[5:]
    pair = []

    def finish_up():
        from_across(0, everything + late)
        up = up_out[...].reshape(shards * rows, width)
        hidden = jnp.dot(normed[...], up, preferred_element_type=jnp.float32)
        active[...] = jnp.square(jnp.maximum(hidden, 0.0)).astype(jnp.bfloat16)

    def far_sums():
        from_across(1, far)
        for slot in range(cut):
            part_of(slot)
        pair.append(exchange(0, 0, cut))

    events = []
    for n in range(sources):
        events.append((6.5 + 1.6 * n, to_sides, 0, n))
        events.append((6.5 + behind + 1.6 * n, from_sides, 0, n))
    for n, i in enumerate(late):
        events.append((16.0 + n, to_sides, 0, i))
        events.append((16.0 + behind + n, from_sides, 0, i))
        events.append((24.4 + 0.5 * n, to_sides, 1, i))
        events.append((24.4 + behind + 0.1 * n, from_sides, 1, i))
    for n, i in enumerate(beyond):
        events.append((19.0 + 1.2 * n, to_sides, 1, i))
        events.append((19.0 + behind + 1.2 * n, from_sides, 1, i))
    events.append((24.95 + behind, lambda *_: finish_up(), 0, 0))
    events.append((26.2 + behind, lambda *_: far_sums(), 0, 0))
    for _, act, kind, i in sorted(events, key=lambda event: event[0]):
        act(kind, i)
    pair[0].wait_recv()
    leaves = [(0, top_d, 6), (0, 7, 6), (1, 7, 6), (0, 5, 4), (1, 5, 4)]
    for side, d, target in leaves:
        settle(side, d)
    for side, d, target in leaves:
        pass_on(side, d, target)
    from_across(1, close)
    settle(0, 6, (top_d, 7))
    settle(1, 6, (7,))
    pass_on(0, 6, 3)
    pass_on(1, 6, 3)
    settle(0, 4, (5,))
    settle(1, 4, (5,))
    pass_on(0, 4, 3)
    pass_on(1, 4, 3)
    for slot in range(cut, n_z):
        part_of(slot)
    pair_near = exchange(1, cut, n_z)
    pair_near.wait_recv()
    for d in (2, 1):
        for side in range(2):
            settle(side, d)
    for d in (2, 1):
        for side in range(2):
            pass_on(side, d, 0)
    for side in range(2):
        settle(side, 3, (6, 4))
        pass_on(side, 3, 0)
    home = n_z - 1
    total = mine[home] + got[home].astype(jnp.float32)
    for d in (1, 2, 3):
        for side in range(2):
            j = stage_at[(side, d)]
            pltpu.make_async_copy(stage.at[j], stage.at[j], stage_recv.at[j]).wait()
            total = total + stage[j].astype(jnp.float32)
    total = total.T
    y_ref[:, 0:half] = total[0:rows].astype(jnp.bfloat16)
    y_ref[:, half : 2 * half] = total[rows : 2 * rows].astype(jnp.bfloat16)

    for when, copy in pending:
        if when is None or when is True:
            copy.wait_send()
        else:
            pl.when(when)(copy.wait_send)


def local(shards, planes, tokens, norm_gain, up_trained, down_trained):
    rows, cols = up_trained.shape
    count, depth = tokens.shape
    width = cols * planes // shards
    per_plane = cols // width // planes
    n_z = shards // 2
    half = count // 2
    bf16, f32 = jnp.bfloat16, jnp.float32
    served = pltpu.VMEM((shards, rows, width), bf16)
    dma = pltpu.SemaphoreType.DMA
    any_space = pl.BlockSpec(memory_space=pl.ANY)
    up, down, y = pl.pallas_call(
        functools.partial(kernel, shards, planes),
        out_shape=(served, served, jax.ShapeDtypeStruct((rows, count), bf16)),
        in_specs=[any_space] * 4,
        out_specs=(pl.BlockSpec(memory_space=pltpu.VMEM),) * 3,
        scratch_shapes=[
            pltpu.VMEM((count, depth), bf16),
            pltpu.VMEM((1, rows), f32),
            pltpu.VMEM((2, rows, cols), f32),
            pltpu.VMEM((count, depth), bf16),
            pltpu.VMEM((2, planes, per_plane, rows, width), bf16),
            pltpu.VMEM((2, planes, per_plane, rows, width), bf16),
            pltpu.VMEM((n_z, half, 2 * rows), f32),
            pltpu.VMEM((n_z, half, 2 * rows), bf16),
            pltpu.VMEM((n_z, half, 2 * rows), bf16),
            pltpu.VMEM((n_z, half, 2 * rows), bf16),
            pltpu.VMEM((n_z, half, 2 * rows), bf16),
            dma((4,)),
            dma((2, planes - 1, per_plane)),
            dma((2, planes, per_plane)),
            dma((2, planes * per_plane + per_plane)),
            dma((2, shards)),
            dma((2, shards // planes * 5 // 4, 2)),
            dma((2, shards // planes * 5 // 4, 2)),
            dma((2,)),
            dma((2,)),
            dma((n_z,)),
            dma((n_z,)),
            pltpu.SemaphoreType.REGULAR,
            pltpu.SemaphoreType.REGULAR((shards,)),
            pltpu.VMEM((count, width), bf16),
        ],
        compiler_params=pltpu.CompilerParams(
            collective_id=0, has_side_effects=True, vmem_limit_bytes=61 * 1024 * 1024
        ),
        name="handoff",
    )(tokens, norm_gain.reshape(1, rows), up_trained, down_trained)
    return (up.reshape(shards * rows, width), down.reshape(shards * rows, width), y.T)


def solution(mesh):
    in_specs = (P(("grp", "tp"), None), P("fs"), P("fs", "tp"), P("fs", "tp"))
    out_specs = (P("grp", "fs"), P("grp", "fs"), P(("grp", "tp"), "fs"))
    body = functools.partial(local, mesh.shape["fs"], mesh.shape["tp"])
    return jax.shard_map(body, mesh=mesh, in_specs=in_specs, out_specs=out_specs, check_vma=False)
```

```python
import functools

import jax
import jax.numpy as jnp
from jax import lax
from jax.experimental import pallas as pl
from jax.experimental.pallas import tpu as pltpu
from jax.sharding import PartitionSpec as P

MESH = pl.DeviceIdType.MESH
epsilon = 1e-06
behind = 5.0


def ring_order(n):
    half = n // 2
    far = [d for d in range(half - 1, 3, -1)]
    slots, first = [half], {half: 0}
    for d in far + [2, 1, 3]:
        first[d] = len(slots)
        slots += [d, n - d]
    slots.append(0)
    return slots, first, 1 + 2 * len(far)


def kernel(
    shards,
    planes,
    tok_hbm,
    gain_hbm,
    up_hbm,
    down_hbm,
    up_out,
    down_out,
    y_ref,
    tok,
    gain,
    raw,
    normed,
    src,
    relay,
    mine,
    give,
    got,
    sums,
    stage,
    in_sem,
    p1_send,
    p1_recv,
    p2_send,
    full_recv,
    p3_send,
    p4_send,
    pair_send,
    pair_recv,
    sum_send,
    stage_recv,
    token,
    ready,
    active,
):
    f = lax.axis_index("fs")
    x = lax.axis_index("tp")
    n_z = shards // 2
    z = f // 2
    c = f % 2
    rows, width = up_out.shape[1], up_out.shape[2]

    full = (up_out, down_out)

    def when(flag):
        return (lambda body: body()) if flag is True else pl.when(flag)

    def both(a, b):
        return b if a is True else jnp.logical_and(a, b)

    def around(v, n):
        v = jnp.where(v >= n, v - n, v)
        return jnp.where(v < 0, v + n, v)

    per_plane = src.shape[2]
    blocks_here = planes * per_plane
    sources = shards // planes

    last = n_z - 1
    barrier = pltpu.get_barrier_semaphore()
    for step in range(1, planes):
        pl.semaphore_signal(barrier, inc=1, device_id={"tp": around(x + step, planes)}, device_id_type=MESH)
    pl.semaphore_signal(barrier, inc=1, device_id={"fs": f + 1 - 2 * c}, device_id_type=MESH)

    def greet(at, carry):
        @pl.when(jnp.logical_or(jnp.logical_and(z > 0, at > z), jnp.logical_and(z == 0, at == last)))
        def _():
            for core in range(2):
                pl.semaphore_signal(barrier, inc=1, device_id={"fs": 2 * at + core}, device_id_type=MESH)

        return carry

    lax.fori_loop(1, n_z, greet, 0)

    loads = [
        pltpu.make_async_copy(gain_hbm, gain, in_sem.at[0]),
        pltpu.make_async_copy(up_hbm, raw.at[0], in_sem.at[1]),
        pltpu.make_async_copy(down_hbm, raw.at[1], in_sem.at[2]),
        pltpu.make_async_copy(tok_hbm, tok, in_sem.at[3]),
    ]
    for load in loads:
        load.start()

    turn = (shards * planes - z - 2 * c) % planes

    def first_block(plane):
        return around(plane + turn, planes)

    loads[0].wait()
    row_at = lax.broadcasted_iota(jnp.int32, (rows, rows), 0)
    col_at = lax.broadcasted_iota(jnp.int32, (rows, rows), 1)
    column = jnp.sum(
        jnp.where(row_at == col_at, jnp.broadcast_to(gain[...], (rows, rows)), 0.0), axis=1, keepdims=True
    )

    def fold(kind):
        loads[1 + kind].wait()
        for step in (1, 3, 2, 0):
            plane = around(x + step, planes)
            for b in range(per_plane):
                at = pl.multiple_of((planes * b + first_block(plane)) * width, width)
                block = raw[kind, :, pl.ds(at, width)]
                if kind == 0:
                    block = block * column
                src[kind, plane, b] = block.astype(jnp.bfloat16)

    def norm():
        loads[3].wait()
        step_rows = 64
        for r in range(0, tok.shape[0], step_rows):
            values = tok[r : r + step_rows, :].astype(jnp.float32)
            scale = lax.rsqrt(jnp.mean(values * values, axis=1, keepdims=True) + epsilon)
            normed[r : r + step_rows, :] = (values * scale).astype(jnp.bfloat16)

    lower = jnp.where(z > 0, 2 * (z - 1), 0) + jnp.where(z == last, 2, 0)
    pl.semaphore_wait(barrier, planes + lower)

    @pl.when(z == last)
    def _():
        pl.semaphore_signal(token, inc=1, device_id={"fs": f - 2 * last}, device_id_type=MESH)


    pending = []

    def spread(kind):
        fold(kind)
        for b in range(per_plane):
            for step in (1, 3, 2):
                plane = around(x + step, planes)
                copy = pltpu.make_async_remote_copy(
                    src_ref=src.at[kind, plane, b],
                    dst_ref=relay.at[kind, x, b],
                    send_sem=p1_send.at[kind, step - 1, b],
                    recv_sem=p1_recv.at[kind, x, b],
                    device_id={"tp": plane},
                    device_id_type=MESH,
                )
                copy.start()
                pending.append((None, copy))
        relay[kind, x] = src[kind, x]

    hops = [2 * ((i + 1) // 2) if i % 2 == 0 else -2 * ((i + 1) // 2) for i in range(sources)]

    def turn_of(plane):
        return (plane + 2 * shards - f) % planes

    def sources_of(plane):
        r = turn_of(plane)
        odd = (z + r) % 2
        base = ((z + odd + planes - r) // 2) % 2
        found = []
        for ahead in hops:
            core = base if (ahead // 2) % 2 == 0 else 1 - base
            found.append(2 * around(z + odd + ahead, n_z) + core)
        return found

    own, right, across, left = [sources_of(around(x + step, planes)) for step in range(planes)]
    beyond = list(range(sources - 1, -1, -1))
    def tell():
        for at in own:

            @pl.when(jnp.logical_and(at >= 2, jnp.logical_or(at < 2 * z, z == 0)))
            def _():
                pl.semaphore_signal(ready.at[f], inc=1, device_id={"fs": at}, device_id_type=MESH)

    pl.when(z > 0)(tell)
    spread(0)
    spread(1)

    @pl.when(z == 0)
    def _():
        pl.semaphore_wait(token, 1)
        tell()

    s = first_block(x)
    lift = s // 2

    def taken(kind, a, b):
        here = relay.at[kind, a, b]
        pltpu.make_async_copy(here, here, p1_recv.at[kind, a, b]).wait()

    def along(kind, a, b, n, wanted=True):
        to = blocks_here * a + planes * b + s
        away = both(wanted, to != f)
        held = relay.at[kind, a, b]
        copy = pltpu.make_async_remote_copy(
            src_ref=held,
            dst_ref=full[kind].at[f],
            send_sem=p2_send.at[kind, n],
            recv_sem=full_recv.at[kind, f],
            device_id={"fs": to},
            device_id_type=MESH,
        )
        pl.when(both(wanted, a != x))(lambda: taken(kind, a, b))
        if kind == 0:

            @pl.when(both(wanted, jnp.logical_and(z > 0, jnp.logical_or(to > 2 * z + 1, to < 2))))
            def _():
                pl.semaphore_wait(ready.at[to], 1)

        pl.when(away)(copy.start)
        pending.append((away, copy))

        @pl.when(both(wanted, to == f))
        def _():
            full[kind][f] = held[...]

    norm()

    def arrived(kind, at):
        return pltpu.make_async_copy(full[kind].at[at], full[kind].at[at], full_recv.at[kind, at])

    def forward(kind, at, step, sem):
        copy = pltpu.make_async_remote_copy(
            src_ref=full[kind].at[at],
            dst_ref=full[kind].at[at],
            send_sem=sem,
            recv_sem=full_recv.at[kind, at],
            device_id={"tp": around(x + step, planes)},
            device_id_type=MESH,
        )
        return copy

    early = n_z - n_z // 4
    late = list(range(sources, sources + sources // 4))

    def of_slot(step, i):
        if i < sources:
            at = (own, right, across, left)[step][i]
            return at, jnp.logical_and(at >= 2, at < 2 * early + 2)
        r = turn_of(around(x + step, planes))
        zs = around(early + 1 + 2 * (i - sources) + (r + early + 1) % 2, n_z)
        return 2 * zs + ((zs + planes - r) // 2) % 2, True

    def to_sides(kind, i):
        at, stands = of_slot(0, i)

        @when(stands)
        def _():
            pl.when(at != f)(lambda: arrived(kind, at).wait())
            forward(kind, at, 1, p3_send.at[kind, i, 0]).start()
            forward(kind, at, 3, p3_send.at[kind, i, 1]).start()

        pending.append((stands, forward(kind, at, 1, p3_send.at[kind, i, 0])))
        pending.append((stands, forward(kind, at, 3, p3_send.at[kind, i, 1])))

    def from_sides(kind, i):
        for from_step, to_step, parity in ((3, 1, 0), (1, 3, 1)):
            at, stands = of_slot(from_step, i)
            turned = (at // 4) % 2 == parity
            sem = p4_send.at[kind, i, parity]

            @when(stands)
            def _():
                arrived(kind, at).wait()
                pl.when(turned)(lambda: forward(kind, at, to_step, sem).start())

            pending.append((both(stands, turned), forward(kind, at, to_step, sem)))

    def from_across(kind, some):
        for i in some:
            at, stands = of_slot(2, i)
            when(stands)(lambda: arrived(kind, at).wait())

    near = z + jnp.where(z < lift, lift - z, z - lift) % 2
    everything = list(range(sources))
    for b in range(per_plane):
        along(0, x, b, sources + b)
    for kind, some in ((0, everything), (1, beyond)):
        for i in some:
            k = (around(near + hops[i], n_z) - lift) // 2
            a = k // per_plane
            along(kind, a, k % per_plane, i, a != x if kind == 0 else True)

    half = tok.shape[0] // 2
    low = lax.broadcasted_iota(jnp.int32, (half, 2 * rows), 1) < rows
    slots, first, cut = ring_order(n_z)

    def part_of(slot):
        owner = around(z + slots[slot], n_z)
        block = down_out[pl.ds(2 * owner, 2)].reshape(2 * rows, width)
        part = lax.dot_general(active[...], block, (((1,), (1,)), ((), ())), preferred_element_type=jnp.float32)
        top, bottom = part[:half], part[half:]
        even = jnp.where(low, top, pltpu.roll(bottom, rows, 1))
        odd = jnp.where(low, pltpu.roll(top, rows, 1), bottom)
        mine[slot] = jnp.where(c == 0, even, odd)
        give[slot] = jnp.where(c == 0, odd, even).astype(jnp.bfloat16)

    def exchange(j, start, stop):
        copy = pltpu.make_async_remote_copy(
            src_ref=give.at[pl.ds(start, stop - start)],
            dst_ref=got.at[pl.ds(start, stop - start)],
            send_sem=pair_send.at[j],
            recv_sem=pair_recv.at[j],
            device_id={"fs": f + 1 - 2 * c},
            device_id_type=MESH,
        )
        copy.start()
        pending.append((None, copy))
        return copy

    top_d = n_z // 2
    sign = 1 - 2 * c

    def place(side, d):
        if d == top_d:
            return 0
        return first[d] + (c if side == 0 else 1 - c)

    count = [0]
    stage_at = {}

    def pass_on(side, d, target):
        j = count[0]
        count[0] += 1
        stage_at[(side, d)] = j
        to = around(z + (sign if side == 0 else -sign) * (d - target), n_z)
        copy = pltpu.make_async_remote_copy(
            src_ref=sums.at[place(side, d)],
            dst_ref=stage.at[j],
            send_sem=sum_send.at[j],
            recv_sem=stage_recv.at[j],
            device_id={"fs": 2 * to + c},
            device_id_type=MESH,
        )
        copy.start()
        pending.append((None, copy))

    def add_up(side, d, below):
        slot = place(side, d)
        total = mine[slot] + got[slot].astype(jnp.float32)
        for e in below:
            j = stage_at[(side, e)]
            pltpu.make_async_copy(stage.at[j], stage.at[j], stage_recv.at[j]).wait()
            total = total + stage[j].astype(jnp.float32)
        return total

    def settle(side, d, below=()):
        sums[place(side, d)] = add_up(side, d, below).astype(jnp.bfloat16)

    far = beyond[:5] + late
    close = beyond[5:]
    pair = []

    def finish_up():
        from_across(0, everything + late)
        up = up_out[...].reshape(shards * rows, width)
        hidden = jnp.dot(normed[...], up, preferred_element_type=jnp.float32)
        active[...] = jnp.square(jnp.maximum(hidden, 0.0)).astype(jnp.bfloat16)

    def far_sums():
        from_across(1, far)
        for slot in range(cut):
            part_of(slot)
        pair.append(exchange(0, 0, cut))

    events = []
    for n in range(sources):
        events.append((6.5 + 1.6 * n, to_sides, 0, n))
        events.append((6.5 + behind + 1.6 * n, from_sides, 0, n))
    for n, i in enumerate(late):
        events.append((16.0 + n, to_sides, 0, i))
        events.append((16.0 + behind + n, from_sides, 0, i))
        events.append((24.4 + 0.5 * n, to_sides, 1, i))
        events.append((24.4 + behind + 0.1 * n, from_sides, 1, i))
    for n, i in enumerate(beyond):
        events.append((19.0 + 1.2 * n, to_sides, 1, i))
        events.append((19.0 + behind + 1.2 * n, from_sides, 1, i))
    events.append((24.95 + behind, lambda *_: finish_up(), 0, 0))
    events.append((26.2 + behind, lambda *_: far_sums(), 0, 0))
    for _, act, kind, i in sorted(events, key=lambda event: event[0]):
        act(kind, i)
    pair[0].wait_recv()
    leaves = [(0, top_d, 6), (0, 7, 6), (1, 7, 6), (0, 5, 4), (1, 5, 4)]
    for side, d, target in leaves:
        settle(side, d)
    for side, d, target in leaves:
        pass_on(side, d, target)
    from_across(1, close)
    settle(0, 6, (top_d, 7))
    settle(1, 6, (7,))
    pass_on(0, 6, 3)
    pass_on(1, 6, 3)
    settle(0, 4, (5,))
    settle(1, 4, (5,))
    pass_on(0, 4, 3)
    pass_on(1, 4, 3)
    for slot in range(cut, n_z):
        part_of(slot)
    pair_near = exchange(1, cut, n_z)
    pair_near.wait_recv()
    for d in (2, 1):
        for side in range(2):
            settle(side, d)
    for d in (2, 1):
        for side in range(2):
            pass_on(side, d, 0)
    for side in range(2):
        settle(side, 3, (6, 4))
        pass_on(side, 3, 0)
    home = n_z - 1
    total = mine[home] + got[home].astype(jnp.float32)
    for d in (1, 2, 3):
        for side in range(2):
            j = stage_at[(side, d)]
            pltpu.make_async_copy(stage.at[j], stage.at[j], stage_recv.at[j]).wait()
            total = total + stage[j].astype(jnp.float32)
    total = total.T
    y_ref[:, 0:half] = total[0:rows].astype(jnp.bfloat16)
    y_ref[:, half : 2 * half] = total[rows : 2 * rows].astype(jnp.bfloat16)

    for when, copy in pending:
        if when is None or when is True:
            copy.wait_send()
        else:
            pl.when(when)(copy.wait_send)


def local(shards, planes, tokens, norm_gain, up_trained, down_trained):
    rows, cols = up_trained.shape
    count, depth = tokens.shape
    width = cols * planes // shards
    per_plane = cols // width // planes
    n_z = shards // 2
    half = count // 2
    bf16, f32 = jnp.bfloat16, jnp.float32
    served = pltpu.VMEM((shards, rows, width), bf16)
    dma = pltpu.SemaphoreType.DMA
    any_space = pl.BlockSpec(memory_space=pl.ANY)
    up, down, y = pl.pallas_call(
        functools.partial(kernel, shards, planes),
        out_shape=(served, served, jax.ShapeDtypeStruct((rows, count), bf16)),
        in_specs=[any_space] * 4,
        out_specs=(pl.BlockSpec(memory_space=pltpu.VMEM),) * 3,
        scratch_shapes=[
            pltpu.VMEM((count, depth), bf16),
            pltpu.VMEM((1, rows), f32),
            pltpu.VMEM((2, rows, cols), f32),
            pltpu.VMEM((count, depth), bf16),
            pltpu.VMEM((2, planes, per_plane, rows, width), bf16),
            pltpu.VMEM((2, planes, per_plane, rows, width), bf16),
            pltpu.VMEM((n_z, half, 2 * rows), f32),
            pltpu.VMEM((n_z, half, 2 * rows), bf16),
            pltpu.VMEM((n_z, half, 2 * rows), bf16),
            pltpu.VMEM((n_z, half, 2 * rows), bf16),
            pltpu.VMEM((n_z, half, 2 * rows), bf16),
            dma((4,)),
            dma((2, planes - 1, per_plane)),
            dma((2, planes, per_plane)),
            dma((2, planes * per_plane + per_plane)),
            dma((2, shards)),
            dma((2, shards // planes * 5 // 4, 2)),
            dma((2, shards // planes * 5 // 4, 2)),
            dma((2,)),
            dma((2,)),
            dma((n_z,)),
            dma((n_z,)),
            pltpu.SemaphoreType.REGULAR,
            pltpu.SemaphoreType.REGULAR((shards,)),
            pltpu.VMEM((count, width), bf16),
        ],
        compiler_params=pltpu.CompilerParams(
            collective_id=0, has_side_effects=True, vmem_limit_bytes=61 * 1024 * 1024
        ),
        name="handoff",
    )(tokens, norm_gain.reshape(1, rows), up_trained, down_trained)
    return (up.reshape(shards * rows, width), down.reshape(shards * rows, width), y.T)


def solution(mesh):
    in_specs = (P(("grp", "tp"), None), P("fs"), P("fs", "tp"), P("fs", "tp"))
    out_specs = (P("grp", "fs"), P("grp", "fs"), P(("grp", "tp"), "fs"))
    body = functools.partial(local, mesh.shape["fs"], mesh.shape["tp"])
    return jax.shard_map(body, mesh=mesh, in_specs=in_specs, out_specs=out_specs, check_vma=False)
```

```python
import functools

import jax
import jax.numpy as jnp
from jax import lax
from jax.experimental import pallas as pl
from jax.experimental.pallas import tpu as pltpu
from jax.sharding import PartitionSpec as P

MESH = pl.DeviceIdType.MESH
epsilon = 1e-06
behind = 8.0


def ring_order(n):
    half = n // 2
    far = [d for d in range(half - 1, 3, -1)]
    slots, first = [half], {half: 0}
    for d in far + [2, 1, 3]:
        first[d] = len(slots)
        slots += [d, n - d]
    slots.append(0)
    return slots, first, 1 + 2 * len(far)


def kernel(
    shards,
    planes,
    tok_hbm,
    gain_hbm,
    up_hbm,
    down_hbm,
    up_out,
    down_out,
    y_ref,
    tok,
    gain,
    raw,
    normed,
    src,
    relay,
    mine,
    give,
    got,
    sums,
    stage,
    in_sem,
    p1_send,
    p1_recv,
    p2_send,
    full_recv,
    p3_send,
    p4_send,
    pair_send,
    pair_recv,
    sum_send,
    stage_recv,
    token,
    ready,
    active,
):
    f = lax.axis_index("fs")
    x = lax.axis_index("tp")
    n_z = shards // 2
    z = f // 2
    c = f % 2
    rows, width = up_out.shape[1], up_out.shape[2]

    full = (up_out, down_out)

    def when(flag):
        return (lambda body: body()) if flag is True else pl.when(flag)

    def both(a, b):
        return b if a is True else jnp.logical_and(a, b)

    def around(v, n):
        v = jnp.where(v >= n, v - n, v)
        return jnp.where(v < 0, v + n, v)

    per_plane = src.shape[2]
    blocks_here = planes * per_plane
    sources = shards // planes

    last = n_z - 1
    barrier = pltpu.get_barrier_semaphore()
    for step in range(1, planes):
        pl.semaphore_signal(barrier, inc=1, device_id={"tp": around(x + step, planes)}, device_id_type=MESH)
    pl.semaphore_signal(barrier, inc=1, device_id={"fs": f + 1 - 2 * c}, device_id_type=MESH)

    def greet(at, carry):
        @pl.when(jnp.logical_or(jnp.logical_and(z > 0, at > z), jnp.logical_and(z == 0, at == last)))
        def _():
            for core in range(2):
                pl.semaphore_signal(barrier, inc=1, device_id={"fs": 2 * at + core}, device_id_type=MESH)

        return carry

    lax.fori_loop(1, n_z, greet, 0)

    loads = [
        pltpu.make_async_copy(gain_hbm, gain, in_sem.at[0]),
        pltpu.make_async_copy(up_hbm, raw.at[0], in_sem.at[1]),
        pltpu.make_async_copy(down_hbm, raw.at[1], in_sem.at[2]),
        pltpu.make_async_copy(tok_hbm, tok, in_sem.at[3]),
    ]
    for load in loads:
        load.start()

    turn = (shards * planes - z - 2 * c) % planes

    def first_block(plane):
        return around(plane + turn, planes)

    loads[0].wait()
    row_at = lax.broadcasted_iota(jnp.int32, (rows, rows), 0)
    col_at = lax.broadcasted_iota(jnp.int32, (rows, rows), 1)
    column = jnp.sum(
        jnp.where(row_at == col_at, jnp.broadcast_to(gain[...], (rows, rows)), 0.0), axis=1, keepdims=True
    )

    def fold(kind):
        loads[1 + kind].wait()
        for step in (1, 3, 2, 0):
            plane = around(x + step, planes)
            for b in range(per_plane):
                at = pl.multiple_of((planes * b + first_block(plane)) * width, width)
                block = raw[kind, :, pl.ds(at, width)]
                if kind == 0:
                    block = block * column
                src[kind, plane, b] = block.astype(jnp.bfloat16)

    def norm():
        loads[3].wait()
        step_rows = 64
        for r in range(0, tok.shape[0], step_rows):
            values = tok[r : r + step_rows, :].astype(jnp.float32)
            scale = lax.rsqrt(jnp.mean(values * values, axis=1, keepdims=True) + epsilon)
            normed[r : r + step_rows, :] = (values * scale).astype(jnp.bfloat16)

    lower = jnp.where(z > 0, 2 * (z - 1), 0) + jnp.where(z == last, 2, 0)
    pl.semaphore_wait(barrier, planes + lower)

    @pl.when(z == last)
    def _():
        pl.semaphore_signal(token, inc=1, device_id={"fs": f - 2 * last}, device_id_type=MESH)


    pending = []

    def spread(kind):
        fold(kind)
        for b in range(per_plane):
            for step in (1, 3, 2):
                plane = around(x + step, planes)
                copy = pltpu.make_async_remote_copy(
                    src_ref=src.at[kind, plane, b],
                    dst_ref=relay.at[kind, x, b],
                    send_sem=p1_send.at[kind, step - 1, b],
                    recv_sem=p1_recv.at[kind, x, b],
                    device_id={"tp": plane},
                    device_id_type=MESH,
                )
                copy.start()
                pending.append((None, copy))
        relay[kind, x] = src[kind, x]

    hops = [2 * ((i + 1) // 2) if i % 2 == 0 else -2 * ((i + 1) // 2) for i in range(sources)]

    def turn_of(plane):
        return (plane + 2 * shards - f) % planes

    def sources_of(plane):
        r = turn_of(plane)
        odd = (z + r) % 2
        base = ((z + odd + planes - r) // 2) % 2
        found = []
        for ahead in hops:
            core = base if (ahead // 2) % 2 == 0 else 1 - base
            found.append(2 * around(z + odd + ahead, n_z) + core)
        return found

    own, right, across, left = [sources_of(around(x + step, planes)) for step in range(planes)]
    beyond = list(range(sources - 1, -1, -1))
    def tell():
        for at in own:

            @pl.when(jnp.logical_and(at >= 2, jnp.logical_or(at < 2 * z, z == 0)))
            def _():
                pl.semaphore_signal(ready.at[f], inc=1, device_id={"fs": at}, device_id_type=MESH)

    pl.when(z > 0)(tell)
    spread(0)
    spread(1)

    @pl.when(z == 0)
    def _():
        pl.semaphore_wait(token, 1)
        tell()

    s = first_block(x)
    lift = s // 2

    def taken(kind, a, b):
        here = relay.at[kind, a, b]
        pltpu.make_async_copy(here, here, p1_recv.at[kind, a, b]).wait()

    def along(kind, a, b, n, wanted=True):
        to = blocks_here * a + planes * b + s
        away = both(wanted, to != f)
        held = relay.at[kind, a, b]
        copy = pltpu.make_async_remote_copy(
            src_ref=held,
            dst_ref=full[kind].at[f],
            send_sem=p2_send.at[kind, n],
            recv_sem=full_recv.at[kind, f],
            device_id={"fs": to},
            device_id_type=MESH,
        )
        pl.when(both(wanted, a != x))(lambda: taken(kind, a, b))
        if kind == 0:

            @pl.when(both(wanted, jnp.logical_and(z > 0, jnp.logical_or(to > 2 * z + 1, to < 2))))
            def _():
                pl.semaphore_wait(ready.at[to], 1)

        pl.when(away)(copy.start)
        pending.append((away, copy))

        @pl.when(both(wanted, to == f))
        def _():
            full[kind][f] = held[...]

    norm()

    def arrived(kind, at):
        return pltpu.make_async_copy(full[kind].at[at], full[kind].at[at], full_recv.at[kind, at])

    def forward(kind, at, step, sem):
        copy = pltpu.make_async_remote_copy(
            src_ref=full[kind].at[at],
            dst_ref=full[kind].at[at],
            send_sem=sem,
            recv_sem=full_recv.at[kind, at],
            device_id={"tp": around(x + step, planes)},
            device_id_type=MESH,
        )
        return copy

    early = n_z - n_z // 4
    late = list(range(sources, sources + sources // 4))

    def of_slot(step, i):
        if i < sources:
            at = (own, right, across, left)[step][i]
            return at, jnp.logical_and(at >= 2, at < 2 * early + 2)
        r = turn_of(around(x + step, planes))
        zs = around(early + 1 + 2 * (i - sources) + (r + early + 1) % 2, n_z)
        return 2 * zs + ((zs + planes - r) // 2) % 2, True

    def to_sides(kind, i):
        at, stands = of_slot(0, i)

        @when(stands)
        def _():
            pl.when(at != f)(lambda: arrived(kind, at).wait())
            forward(kind, at, 1, p3_send.at[kind, i, 0]).start()
            forward(kind, at, 3, p3_send.at[kind, i, 1]).start()

        pending.append((stands, forward(kind, at, 1, p3_send.at[kind, i, 0])))
        pending.append((stands, forward(kind, at, 3, p3_send.at[kind, i, 1])))

    def from_sides(kind, i):
        for from_step, to_step, parity in ((3, 1, 0), (1, 3, 1)):
            at, stands = of_slot(from_step, i)
            turned = (at // 4) % 2 == parity
            sem = p4_send.at[kind, i, parity]

            @when(stands)
            def _():
                arrived(kind, at).wait()
                pl.when(turned)(lambda: forward(kind, at, to_step, sem).start())

            pending.append((both(stands, turned), forward(kind, at, to_step, sem)))

    def from_across(kind, some):
        for i in some:
            at, stands = of_slot(2, i)
            when(stands)(lambda: arrived(kind, at).wait())

    near = z + jnp.where(z < lift, lift - z, z - lift) % 2
    everything = list(range(sources))
    for b in range(per_plane):
        along(0, x, b, sources + b)
    for kind, some in ((0, everything), (1, beyond)):
        for i in some:
            k = (around(near + hops[i], n_z) - lift) // 2
            a = k // per_plane
            along(kind, a, k % per_plane, i, a != x if kind == 0 else True)

    half = tok.shape[0] // 2
    low = lax.broadcasted_iota(jnp.int32, (half, 2 * rows), 1) < rows
    slots, first, cut = ring_order(n_z)

    def part_of(slot):
        owner = around(z + slots[slot], n_z)
        block = down_out[pl.ds(2 * owner, 2)].reshape(2 * rows, width)
        part = lax.dot_general(active[...], block, (((1,), (1,)), ((), ())), preferred_element_type=jnp.float32)
        top, bottom = part[:half], part[half:]
        even = jnp.where(low, top, pltpu.roll(bottom, rows, 1))
        odd = jnp.where(low, pltpu.roll(top, rows, 1), bottom)
        mine[slot] = jnp.where(c == 0, even, odd)
        give[slot] = jnp.where(c == 0, odd, even).astype(jnp.bfloat16)

    def exchange(j, start, stop):
        copy = pltpu.make_async_remote_copy(
            src_ref=give.at[pl.ds(start, stop - start)],
            dst_ref=got.at[pl.ds(start, stop - start)],
            send_sem=pair_send.at[j],
            recv_sem=pair_recv.at[j],
            device_id={"fs": f + 1 - 2 * c},
            device_id_type=MESH,
        )
        copy.start()
        pending.append((None, copy))
        return copy

    top_d = n_z // 2
    sign = 1 - 2 * c

    def place(side, d):
        if d == top_d:
            return 0
        return first[d] + (c if side == 0 else 1 - c)

    count = [0]
    stage_at = {}

    def pass_on(side, d, target):
        j = count[0]
        count[0] += 1
        stage_at[(side, d)] = j
        to = around(z + (sign if side == 0 else -sign) * (d - target), n_z)
        copy = pltpu.make_async_remote_copy(
            src_ref=sums.at[place(side, d)],
            dst_ref=stage.at[j],
            send_sem=sum_send.at[j],
            recv_sem=stage_recv.at[j],
            device_id={"fs": 2 * to + c},
            device_id_type=MESH,
        )
        copy.start()
        pending.append((None, copy))

    def add_up(side, d, below):
        slot = place(side, d)
        total = mine[slot] + got[slot].astype(jnp.float32)
        for e in below:
            j = stage_at[(side, e)]
            pltpu.make_async_copy(stage.at[j], stage.at[j], stage_recv.at[j]).wait()
            total = total + stage[j].astype(jnp.float32)
        return total

    def settle(side, d, below=()):
        sums[place(side, d)] = add_up(side, d, below).astype(jnp.bfloat16)

    far = beyond[:5] + late
    close = beyond[5:]
    pair = []

    def finish_up():
        from_across(0, everything + late)
        up = up_out[...].reshape(shards * rows, width)
        hidden = jnp.dot(normed[...], up, preferred_element_type=jnp.float32)
        active[...] = jnp.square(jnp.maximum(hidden, 0.0)).astype(jnp.bfloat16)

    def far_sums():
        from_across(1, far)
        for slot in range(cut):
            part_of(slot)
        pair.append(exchange(0, 0, cut))

    events = []
    for n in range(sources):
        events.append((6.5 + 1.6 * n, to_sides, 0, n))
        events.append((6.5 + behind + 1.6 * n, from_sides, 0, n))
    for n, i in enumerate(late):
        events.append((16.0 + n, to_sides, 0, i))
        events.append((16.0 + behind + n, from_sides, 0, i))
        events.append((24.4 + 0.5 * n, to_sides, 1, i))
        events.append((24.4 + behind + 0.1 * n, from_sides, 1, i))
    for n, i in enumerate(beyond):
        events.append((19.0 + 1.2 * n, to_sides, 1, i))
        events.append((19.0 + behind + 1.2 * n, from_sides, 1, i))
    events.append((24.95 + behind, lambda *_: finish_up(), 0, 0))
    events.append((26.2 + behind, lambda *_: far_sums(), 0, 0))
    for _, act, kind, i in sorted(events, key=lambda event: event[0]):
        act(kind, i)
    pair[0].wait_recv()
    leaves = [(0, top_d, 6), (0, 7, 6), (1, 7, 6), (0, 5, 4), (1, 5, 4)]
    for side, d, target in leaves:
        settle(side, d)
    for side, d, target in leaves:
        pass_on(side, d, target)
    from_across(1, close)
    settle(0, 6, (top_d, 7))
    settle(1, 6, (7,))
    pass_on(0, 6, 3)
    pass_on(1, 6, 3)
    settle(0, 4, (5,))
    settle(1, 4, (5,))
    pass_on(0, 4, 3)
    pass_on(1, 4, 3)
    for slot in range(cut, n_z):
        part_of(slot)
    pair_near = exchange(1, cut, n_z)
    pair_near.wait_recv()
    for d in (2, 1):
        for side in range(2):
            settle(side, d)
    for d in (2, 1):
        for side in range(2):
            pass_on(side, d, 0)
    for side in range(2):
        settle(side, 3, (6, 4))
        pass_on(side, 3, 0)
    home = n_z - 1
    total = mine[home] + got[home].astype(jnp.float32)
    for d in (1, 2, 3):
        for side in range(2):
            j = stage_at[(side, d)]
            pltpu.make_async_copy(stage.at[j], stage.at[j], stage_recv.at[j]).wait()
            total = total + stage[j].astype(jnp.float32)
    total = total.T
    y_ref[:, 0:half] = total[0:rows].astype(jnp.bfloat16)
    y_ref[:, half : 2 * half] = total[rows : 2 * rows].astype(jnp.bfloat16)

    for when, copy in pending:
        if when is None or when is True:
            copy.wait_send()
        else:
            pl.when(when)(copy.wait_send)


def local(shards, planes, tokens, norm_gain, up_trained, down_trained):
    rows, cols = up_trained.shape
    count, depth = tokens.shape
    width = cols * planes // shards
    per_plane = cols // width // planes
    n_z = shards // 2
    half = count // 2
    bf16, f32 = jnp.bfloat16, jnp.float32
    served = pltpu.VMEM((shards, rows, width), bf16)
    dma = pltpu.SemaphoreType.DMA
    any_space = pl.BlockSpec(memory_space=pl.ANY)
    up, down, y = pl.pallas_call(
        functools.partial(kernel, shards, planes),
        out_shape=(served, served, pltpu.VMEM((rows, count), bf16)),
        in_specs=[any_space] * 4,
        out_specs=(pl.BlockSpec(memory_space=pltpu.VMEM),) * 3,
        scratch_shapes=[
            pltpu.VMEM((count, depth), bf16),
            pltpu.VMEM((1, rows), f32),
            pltpu.VMEM((2, rows, cols), f32),
            pltpu.VMEM((count, depth), bf16),
            pltpu.VMEM((2, planes, per_plane, rows, width), bf16),
            pltpu.VMEM((2, planes, per_plane, rows, width), bf16),
            pltpu.VMEM((n_z, half, 2 * rows), f32),
            pltpu.VMEM((n_z, half, 2 * rows), bf16),
            pltpu.VMEM((n_z, half, 2 * rows), bf16),
            pltpu.VMEM((n_z, half, 2 * rows), bf16),
            pltpu.VMEM((n_z, half, 2 * rows), bf16),
            dma((4,)),
            dma((2, planes - 1, per_plane)),
            dma((2, planes, per_plane)),
            dma((2, planes * per_plane + per_plane)),
            dma((2, shards)),
            dma((2, shards // planes * 5 // 4, 2)),
            dma((2, shards // planes * 5 // 4, 2)),
            dma((2,)),
            dma((2,)),
            dma((n_z,)),
            dma((n_z,)),
            pltpu.SemaphoreType.REGULAR,
            pltpu.SemaphoreType.REGULAR((shards,)),
            pltpu.VMEM((count, width), bf16),
        ],
        compiler_params=pltpu.CompilerParams(
            collective_id=0, has_side_effects=True, vmem_limit_bytes=61 * 1024 * 1024
        ),
        name="handoff",
    )(tokens, norm_gain.reshape(1, rows), up_trained, down_trained)
    return (up.reshape(shards * rows, width), down.reshape(shards * rows, width), y.T)


def solution(mesh):
    in_specs = (P(("grp", "tp"), None), P("fs"), P("fs", "tp"), P("fs", "tp"))
    out_specs = (P("grp", "fs"), P("grp", "fs"), P(("grp", "tp"), "fs"))
    body = functools.partial(local, mesh.shape["fs"], mesh.shape["tp"])
    return jax.shard_map(body, mesh=mesh, in_specs=in_specs, out_specs=out_specs, check_vma=False)
```

```python
import functools

import jax
import jax.numpy as jnp
from jax import lax
from jax.experimental import pallas as pl
from jax.experimental.pallas import tpu as pltpu
from jax.sharding import PartitionSpec as P

MESH = pl.DeviceIdType.MESH
epsilon = 1e-06
behind = 8.0


def ring_order(n):
    half = n // 2
    far = list(range(half - 1, 3, -2)) + list(range(half - 2, 3, -2))
    slots, first = [half], {half: 0}
    for d in far + [2, 1, 3]:
        first[d] = len(slots)
        slots += [d, n - d]
    slots.append(0)
    return slots, first, first[half - 2], 1 + 2 * len(far)


def kernel(
    shards,
    planes,
    tok_hbm,
    gain_hbm,
    up_hbm,
    down_hbm,
    up_out,
    down_out,
    y_ref,
    tok,
    gain,
    raw,
    normed,
    src,
    relay,
    mine,
    give,
    got,
    sums,
    stage,
    in_sem,
    p1_send,
    p1_recv,
    p2_send,
    full_recv,
    p3_send,
    p4_send,
    pair_send,
    pair_recv,
    sum_send,
    stage_recv,
    token,
    ready,
    active,
):
    f = lax.axis_index("fs")
    x = lax.axis_index("tp")
    n_z = shards // 2
    z = f // 2
    c = f % 2
    rows, width = up_out.shape[1], up_out.shape[2]

    full = (up_out, down_out)

    def when(flag):
        return (lambda body: body()) if flag is True else pl.when(flag)

    def both(a, b):
        return b if a is True else jnp.logical_and(a, b)

    def around(v, n):
        v = jnp.where(v >= n, v - n, v)
        return jnp.where(v < 0, v + n, v)

    per_plane = src.shape[2]
    blocks_here = planes * per_plane
    sources = shards // planes

    last = n_z - 1
    barrier = pltpu.get_barrier_semaphore()
    for step in range(1, planes):
        pl.semaphore_signal(barrier, inc=1, device_id={"tp": around(x + step, planes)}, device_id_type=MESH)
    pl.semaphore_signal(barrier, inc=1, device_id={"fs": f + 1 - 2 * c}, device_id_type=MESH)

    def greet(at, carry):
        @pl.when(jnp.logical_or(jnp.logical_and(z > 0, at > z), jnp.logical_and(z == 0, at == last)))
        def _():
            for core in range(2):
                pl.semaphore_signal(barrier, inc=1, device_id={"fs": 2 * at + core}, device_id_type=MESH)

        return carry

    lax.fori_loop(1, n_z, greet, 0)

    loads = [
        pltpu.make_async_copy(gain_hbm, gain, in_sem.at[0]),
        pltpu.make_async_copy(up_hbm, raw.at[0], in_sem.at[1]),
        pltpu.make_async_copy(down_hbm, raw.at[1], in_sem.at[2]),
        pltpu.make_async_copy(tok_hbm, tok, in_sem.at[3]),
    ]
    for load in loads:
        load.start()

    turn = (shards * planes - z - 2 * c) % planes

    def first_block(plane):
        return around(plane + turn, planes)

    loads[0].wait()
    row_at = lax.broadcasted_iota(jnp.int32, (rows, rows), 0)
    col_at = lax.broadcasted_iota(jnp.int32, (rows, rows), 1)
    column = jnp.sum(
        jnp.where(row_at == col_at, jnp.broadcast_to(gain[...], (rows, rows)), 0.0), axis=1, keepdims=True
    )

    def fold(kind):
        loads[1 + kind].wait()
        for step in (1, 3, 2, 0):
            plane = around(x + step, planes)
            for b in range(per_plane):
                at = pl.multiple_of((planes * b + first_block(plane)) * width, width)
                block = raw[kind, :, pl.ds(at, width)]
                if kind == 0:
                    block = block * column
                src[kind, plane, b] = block.astype(jnp.bfloat16)

    def norm():
        loads[3].wait()
        step_rows = 64
        for r in range(0, tok.shape[0], step_rows):
            values = tok[r : r + step_rows, :].astype(jnp.float32)
            scale = lax.rsqrt(jnp.mean(values * values, axis=1, keepdims=True) + epsilon)
            normed[r : r + step_rows, :] = (values * scale).astype(jnp.bfloat16)

    lower = jnp.where(z > 0, 2 * (z - 1), 0) + jnp.where(z == last, 2, 0)
    pl.semaphore_wait(barrier, planes + lower)

    @pl.when(z == last)
    def _():
        pl.semaphore_signal(token, inc=1, device_id={"fs": f - 2 * last}, device_id_type=MESH)


    pending = []

    def spread(kind):
        fold(kind)
        for b in range(per_plane):
            for step in (1, 3, 2):
                plane = around(x + step, planes)
                copy = pltpu.make_async_remote_copy(
                    src_ref=src.at[kind, plane, b],
                    dst_ref=relay.at[kind, x, b],
                    send_sem=p1_send.at[kind, step - 1, b],
                    recv_sem=p1_recv.at[kind, x, b],
                    device_id={"tp": plane},
                    device_id_type=MESH,
                )
                copy.start()
                pending.append((None, copy))
        relay[kind, x] = src[kind, x]

    hops = [2 * ((i + 1) // 2) if i % 2 == 0 else -2 * ((i + 1) // 2) for i in range(sources)]

    def turn_of(plane):
        return (plane + 2 * shards - f) % planes

    def sources_of(plane):
        r = turn_of(plane)
        odd = (z + r) % 2
        base = ((z + odd + planes - r) // 2) % 2
        found = []
        for ahead in hops:
            core = base if (ahead // 2) % 2 == 0 else 1 - base
            found.append(2 * around(z + odd + ahead, n_z) + core)
        return found

    own, right, across, left = [sources_of(around(x + step, planes)) for step in range(planes)]
    beyond = list(range(sources - 1, -1, -1))
    def tell():
        for at in own:

            @pl.when(jnp.logical_and(at >= 2, jnp.logical_or(at < 2 * z, z == 0)))
            def _():
                pl.semaphore_signal(ready.at[f], inc=1, device_id={"fs": at}, device_id_type=MESH)

    pl.when(z > 0)(tell)
    spread(0)
    spread(1)

    @pl.when(z == 0)
    def _():
        pl.semaphore_wait(token, 1)
        tell()

    s = first_block(x)
    lift = s // 2

    def taken(kind, a, b):
        here = relay.at[kind, a, b]
        pltpu.make_async_copy(here, here, p1_recv.at[kind, a, b]).wait()

    def along(kind, a, b, n, wanted=True):
        to = blocks_here * a + planes * b + s
        away = both(wanted, to != f)
        held = relay.at[kind, a, b]
        copy = pltpu.make_async_remote_copy(
            src_ref=held,
            dst_ref=full[kind].at[f],
            send_sem=p2_send.at[kind, n],
            recv_sem=full_recv.at[kind, f],
            device_id={"fs": to},
            device_id_type=MESH,
        )
        pl.when(both(wanted, a != x))(lambda: taken(kind, a, b))
        if kind == 0:

            @pl.when(both(wanted, jnp.logical_and(z > 0, jnp.logical_or(to > 2 * z + 1, to < 2))))
            def _():
                pl.semaphore_wait(ready.at[to], 1)

        pl.when(away)(copy.start)
        pending.append((away, copy))

        @pl.when(both(wanted, to == f))
        def _():
            full[kind][f] = held[...]

    norm()

    def arrived(kind, at):
        return pltpu.make_async_copy(full[kind].at[at], full[kind].at[at], full_recv.at[kind, at])

    def forward(kind, at, step, sem):
        copy = pltpu.make_async_remote_copy(
            src_ref=full[kind].at[at],
            dst_ref=full[kind].at[at],
            send_sem=sem,
            recv_sem=full_recv.at[kind, at],
            device_id={"tp": around(x + step, planes)},
            device_id_type=MESH,
        )
        return copy

    early = n_z - n_z // 4
    late = list(range(sources, sources + sources // 4))

    def of_slot(step, i):
        if i < sources:
            at = (own, right, across, left)[step][i]
            return at, jnp.logical_and(at >= 2, at < 2 * early + 2)
        r = turn_of(around(x + step, planes))
        zs = around(early + 1 + 2 * (i - sources) + (r + early + 1) % 2, n_z)
        return 2 * zs + ((zs + planes - r) // 2) % 2, True

    def to_sides(kind, i):
        at, stands = of_slot(0, i)

        @when(stands)
        def _():
            pl.when(at != f)(lambda: arrived(kind, at).wait())
            forward(kind, at, 1, p3_send.at[kind, i, 0]).start()
            forward(kind, at, 3, p3_send.at[kind, i, 1]).start()

        pending.append((stands, forward(kind, at, 1, p3_send.at[kind, i, 0])))
        pending.append((stands, forward(kind, at, 3, p3_send.at[kind, i, 1])))

    def from_sides(kind, i):
        for from_step, to_step, parity in ((3, 1, 0), (1, 3, 1)):
            at, stands = of_slot(from_step, i)
            turned = (at // 4) % 2 == parity
            sem = p4_send.at[kind, i, parity]

            @when(stands)
            def _():
                arrived(kind, at).wait()
                pl.when(turned)(lambda: forward(kind, at, to_step, sem).start())

            pending.append((both(stands, turned), forward(kind, at, to_step, sem)))

    def from_across(kind, some):
        for i in some:
            at, stands = of_slot(2, i)
            when(stands)(lambda: arrived(kind, at).wait())

    near = z + jnp.where(z < lift, lift - z, z - lift) % 2
    everything = list(range(sources))
    for b in range(per_plane):
        along(0, x, b, sources + b)
    for kind, some in ((0, everything), (1, beyond)):
        for i in some:
            k = (around(near + hops[i], n_z) - lift) // 2
            a = k // per_plane
            along(kind, a, k % per_plane, i, a != x if kind == 0 else True)

    half = tok.shape[0] // 2
    low = lax.broadcasted_iota(jnp.int32, (half, 2 * rows), 1) < rows
    slots, first, leaf, cut = ring_order(n_z)

    def part_of(slot):
        owner = around(z + slots[slot], n_z)
        block = down_out[pl.ds(2 * owner, 2)].reshape(2 * rows, width)
        part = lax.dot_general(active[...], block, (((1,), (1,)), ((), ())), preferred_element_type=jnp.float32)
        top, bottom = part[:half], part[half:]
        even = jnp.where(low, top, pltpu.roll(bottom, rows, 1))
        odd = jnp.where(low, pltpu.roll(top, rows, 1), bottom)
        mine[slot] = jnp.where(c == 0, even, odd)
        give[slot] = jnp.where(c == 0, odd, even).astype(jnp.bfloat16)

    def exchange(j, start, stop):
        copy = pltpu.make_async_remote_copy(
            src_ref=give.at[pl.ds(start, stop - start)],
            dst_ref=got.at[pl.ds(start, stop - start)],
            send_sem=pair_send.at[j],
            recv_sem=pair_recv.at[j],
            device_id={"fs": f + 1 - 2 * c},
            device_id_type=MESH,
        )
        copy.start()
        pending.append((None, copy))
        return copy

    top_d = n_z // 2
    sign = 1 - 2 * c

    def place(side, d):
        if d == top_d:
            return 0
        return first[d] + (c if side == 0 else 1 - c)

    count = [0]
    stage_at = {}

    def pass_on(side, d, target):
        j = count[0]
        count[0] += 1
        stage_at[(side, d)] = j
        to = around(z + (sign if side == 0 else -sign) * (d - target), n_z)
        copy = pltpu.make_async_remote_copy(
            src_ref=sums.at[place(side, d)],
            dst_ref=stage.at[j],
            send_sem=sum_send.at[j],
            recv_sem=stage_recv.at[j],
            device_id={"fs": 2 * to + c},
            device_id_type=MESH,
        )
        copy.start()
        pending.append((None, copy))

    def add_up(side, d, below):
        slot = place(side, d)
        total = mine[slot] + got[slot].astype(jnp.float32)
        for e in below:
            j = stage_at[(side, e)]
            pltpu.make_async_copy(stage.at[j], stage.at[j], stage_recv.at[j]).wait()
            total = total + stage[j].astype(jnp.float32)
        return total

    def settle(side, d, below=()):
        sums[place(side, d)] = add_up(side, d, below).astype(jnp.bfloat16)

    far = beyond[:5] + late
    close = beyond[5:]
    pair = []

    def finish_up():
        from_across(0, everything + late)
        up = up_out[...].reshape(shards * rows, width)
        hidden = jnp.dot(normed[...], up, preferred_element_type=jnp.float32)
        active[...] = jnp.square(jnp.maximum(hidden, 0.0)).astype(jnp.bfloat16)

    def far_sums():
        from_across(1, far)
        for j, (start, stop) in enumerate(((0, leaf), (leaf, cut))):
            for slot in range(start, stop):
                part_of(slot)
            pair.append(exchange(j, start, stop))

    events = []
    for n in range(sources):
        events.append((6.5 + 1.6 * n, to_sides, 0, n))
        events.append((6.5 + behind + 1.6 * n, from_sides, 0, n))
    for n, i in enumerate(late):
        events.append((16.0 + n, to_sides, 0, i))
        events.append((16.0 + behind + n, from_sides, 0, i))
        events.append((24.4 + 0.5 * n, to_sides, 1, i))
        events.append((24.4 + behind + 0.1 * n, from_sides, 1, i))
    for n, i in enumerate(beyond):
        events.append((19.0 + 1.2 * n, to_sides, 1, i))
        events.append((19.0 + behind + 1.2 * n, from_sides, 1, i))
    events.append((24.95 + behind, lambda *_: finish_up(), 0, 0))
    events.append((26.2 + behind, lambda *_: far_sums(), 0, 0))
    for _, act, kind, i in sorted(events, key=lambda event: event[0]):
        act(kind, i)
    pair[0].wait_recv()
    leaves = [(0, top_d, 6), (0, 7, 6), (1, 7, 6), (0, 5, 4), (1, 5, 4)]
    for side, d, target in leaves:
        settle(side, d)
    for side, d, target in leaves:
        pass_on(side, d, target)
    from_across(1, close)
    pair[1].wait_recv()
    settle(0, 6, (top_d, 7))
    settle(1, 6, (7,))
    pass_on(0, 6, 3)
    pass_on(1, 6, 3)
    settle(0, 4, (5,))
    settle(1, 4, (5,))
    pass_on(0, 4, 3)
    pass_on(1, 4, 3)
    for slot in range(cut, n_z):
        part_of(slot)
    pair_near = exchange(2, cut, n_z)
    pair_near.wait_recv()
    for d in (2, 1):
        for side in range(2):
            settle(side, d)
    for d in (2, 1):
        for side in range(2):
            pass_on(side, d, 0)
    for side in range(2):
        settle(side, 3, (6, 4))
        pass_on(side, 3, 0)
    home = n_z - 1
    total = mine[home] + got[home].astype(jnp.float32)
    for d in (1, 2, 3):
        for side in range(2):
            j = stage_at[(side, d)]
            pltpu.make_async_copy(stage.at[j], stage.at[j], stage_recv.at[j]).wait()
            total = total + stage[j].astype(jnp.float32)
    total = total.T
    y_ref[:, 0:half] = total[0:rows].astype(jnp.bfloat16)
    y_ref[:, half : 2 * half] = total[rows : 2 * rows].astype(jnp.bfloat16)

    for when, copy in pending:
        if when is None or when is True:
            copy.wait_send()
        else:
            pl.when(when)(copy.wait_send)


def local(shards, planes, tokens, norm_gain, up_trained, down_trained):
    rows, cols = up_trained.shape
    count, depth = tokens.shape
    width = cols * planes // shards
    per_plane = cols // width // planes
    n_z = shards // 2
    half = count // 2
    bf16, f32 = jnp.bfloat16, jnp.float32
    served = pltpu.VMEM((shards, rows, width), bf16)
    dma = pltpu.SemaphoreType.DMA
    any_space = pl.BlockSpec(memory_space=pl.ANY)
    up, down, y = pl.pallas_call(
        functools.partial(kernel, shards, planes),
        out_shape=(served, served, pltpu.VMEM((rows, count), bf16)),
        in_specs=[any_space] * 4,
        out_specs=(pl.BlockSpec(memory_space=pltpu.VMEM),) * 3,
        scratch_shapes=[
            pltpu.VMEM((count, depth), bf16),
            pltpu.VMEM((1, rows), f32),
            pltpu.VMEM((2, rows, cols), f32),
            pltpu.VMEM((count, depth), bf16),
            pltpu.VMEM((2, planes, per_plane, rows, width), bf16),
            pltpu.VMEM((2, planes, per_plane, rows, width), bf16),
            pltpu.VMEM((n_z, half, 2 * rows), f32),
            pltpu.VMEM((n_z, half, 2 * rows), bf16),
            pltpu.VMEM((n_z, half, 2 * rows), bf16),
            pltpu.VMEM((n_z, half, 2 * rows), bf16),
            pltpu.VMEM((n_z, half, 2 * rows), bf16),
            dma((4,)),
            dma((2, planes - 1, per_plane)),
            dma((2, planes, per_plane)),
            dma((2, planes * per_plane + per_plane)),
            dma((2, shards)),
            dma((2, shards // planes * 5 // 4, 2)),
            dma((2, shards // planes * 5 // 4, 2)),
            dma((3,)),
            dma((3,)),
            dma((n_z,)),
            dma((n_z,)),
            pltpu.SemaphoreType.REGULAR,
            pltpu.SemaphoreType.REGULAR((shards,)),
            pltpu.VMEM((count, width), bf16),
        ],
        compiler_params=pltpu.CompilerParams(
            collective_id=0, has_side_effects=True, vmem_limit_bytes=61 * 1024 * 1024
        ),
        name="handoff",
    )(tokens, norm_gain.reshape(1, rows), up_trained, down_trained)
    return (up.reshape(shards * rows, width), down.reshape(shards * rows, width), y.T)


def solution(mesh):
    in_specs = (P(("grp", "tp"), None), P("fs"), P("fs", "tp"), P("fs", "tp"))
    out_specs = (P("grp", "fs"), P("grp", "fs"), P(("grp", "tp"), "fs"))
    body = functools.partial(local, mesh.shape["fs"], mesh.shape["tp"])
    return jax.shard_map(body, mesh=mesh, in_specs=in_specs, out_specs=out_specs, check_vma=False)
```
